32 devices in a mesh: sp: 16 (over z, y, x), tp: 2 (over core).
Axes of the slice: x: 2, y: 2, z: 4, core: 2. Of those that a mesh axis runs over, the one named last changes fastest.
Arguments:
- glu_value: bfloat16 [4096, 1024], P('sp', 'tp'), may hold values from -12 to 12
- glu_gate: bfloat16 [4096, 1024], P('sp', 'tp'), may hold values from -8 to 8
- conv_kernel: bfloat16 [31, 1024], P(None, 'tp'), may hold values from -1 to 1
- conv_bias: float32 [1024], P('tp'), may hold values from -1.5 to 1.5
- group_gain: float32 [1024], P('tp'), may hold values from 0.1 to 1.9
- group_shift: float32 [1024], P('tp'), may hold values from -2.5 to 2.5
- out_weight: bfloat16 [1024, 2048], replicated, may hold values from -0.1875 to 0.1875
- residual: bfloat16 [4096, 2048], P(('sp', 'tp')), may hold values from -12 to 12
- ffn_gain: float32 [2048], replicated, may hold values from 0.1 to 1.9
- expert_pick: int32 [4096, 2], P(('sp', 'tp')), may hold values from 0 to 31, as said below
- pair_logits: float32 [4096, 2], P(('sp', 'tp')), may hold values from -1.2 to 1.2
- group_prob: float32 [4096], P(('sp', 'tp')), may hold values from 0.5 to 1
- gate_weight: bfloat16 [32, 2048, 512], P(('sp', 'tp')), may hold values from -0.125 to 0.125
- up_weight: bfloat16 [32, 2048, 512], P(('sp', 'tp')), may hold values from -0.125 to 0.125
- down_weight: bfloat16 [32, 512, 2048], P(('sp', 'tp')), may hold values from -0.75 to 0.75
Outputs:
- result: bfloat16 [4096, 2048], P(('sp', 'tp'))
The draws below stay inside these ranges and needn't reach their ends.
Inputs may be any that keep to these rules, and one draw needn't show every extreme that they name: `expert_pick`: both picks of a token are different experts of the same group of 8 consecutive experts. Among the 128 tokens of one device (aligned blocks of rows) no expert is picked more than 16 times, and in every such block some expert is picked exactly 16 times.
All inputs are finite; a program needn't handle non-finite values.
Results may differ from the reference program's by a relative error of at most 0.014.
Values may be sent and summed in bfloat16 or wider, within the bound.
A program may use at most 64 MiB of HBM per device.

```python
import math
import jax
import jax.numpy as jnp
from jax import lax

D = 2048
CONV = 1024
CONV_GROUPS = 8
KERNEL = 31
FFE = 512
GROUPS = 4
TOK_DEV = 128
TOKENS = 4096
EXPERTS = 32
CAP = 16
N_SP = 16
N_TP = 2


def scaled_normal(key, row_total, columns, lowest, highest):
    subkeys = jax.random.split(key, 3)
    normal_part = jax.random.normal(subkeys[0], (row_total, columns), jnp.float32)
    row_scale = jnp.exp(jax.random.uniform(subkeys[1], (row_total, 1), jnp.float32, jnp.log(lowest), jnp.log(highest)))
    column_scale = jnp.exp(jax.random.uniform(subkeys[2], (1, columns), jnp.float32, jnp.log(lowest), jnp.log(highest)))
    return normal_part * row_scale * column_scale


def draw_residual(key, part):
    scaled = scaled_normal(key, TOKENS, D, 0.2, 2.0)
    return jnp.clip(scaled, -12.0, 12.0).astype(jnp.bfloat16)


def draw_glu_value(key, part):
    scaled = scaled_normal(key, TOKENS, CONV, 0.3, 3.0)
    return jnp.clip(scaled, -12.0, 12.0).astype(jnp.bfloat16)


def draw_expert_pick(key, part):
    per_group = EXPERTS // GROUPS
    pairs = per_group * CAP // 2
    universe = GROUPS * pairs
    blocks = TOKENS // TOK_DEV
    subkeys = jax.random.split(key, 3)
    full_group = jax.random.randint(subkeys[0], (), 0, GROUPS)

    def label_order(label_key):
        return jax.random.permutation(label_key, per_group)
    labels = jax.vmap(label_order)(jax.random.split(subkeys[1], GROUPS)).astype(jnp.int32)
    slot_index = jnp.arange(universe, dtype=jnp.int32)
    slot_group = slot_index // pairs
    slot_pair = slot_index % pairs
    forced = (slot_group == full_group) & (slot_pair < CAP)

    def one_block(block_key):
        inner = jax.random.split(block_key, 3)
        scores = jax.random.randint(inner[0], (universe,), 0, 1 << 18) * universe + slot_index
        scores = jnp.where(forced, slot_pair - CAP, scores)
        chosen = jnp.argsort(scores, stable=True)[:TOK_DEV]
        chosen = chosen[jax.random.permutation(inner[1], TOK_DEV)]
        group_of = slot_group[chosen]
        low_label = slot_pair[chosen] // CAP
        high_label = low_label + per_group // 2
        first_expert = group_of * per_group + labels[group_of, low_label]
        second_expert = group_of * per_group + labels[group_of, high_label]
        flipped = jax.random.randint(inner[2], (TOK_DEV,), 0, 2)
        left_pick = jnp.where(flipped == 1, second_expert, first_expert)
        right_pick = jnp.where(flipped == 1, first_expert, second_expert)
        return jnp.stack([left_pick, right_pick], axis=1)
    picked = jax.vmap(one_block)(jax.random.split(subkeys[2], blocks))
    return picked.reshape(TOKENS, 2).astype(jnp.int32)


def block_scale(key, shape, cuts, low, top_value):
    gain = 1.0
    for position, parts in cuts:
        draws = jax.random.uniform(jax.random.fold_in(jax.random.fold_in(key, 6), position), (parts,), jnp.float32, low / len(cuts), top_value / len(cuts))
        gain = gain * jnp.repeat(jnp.exp(draws), shape[position] // parts).reshape((-1,) + (1,) * (len(shape) - 1 - position))
    return gain


def scatter_about(rng, shape, spread, limit, pieces=(), kind=jnp.bfloat16):
    level = block_scale(rng, shape, pieces, -0.22, 0.18) if pieces else 1.0
    values = jax.random.normal(rng, shape, jnp.float32) * spread * level
    return jnp.minimum(jnp.maximum(values, -limit), limit).astype(kind)


def setup_inputs(seed: int = 0) -> dict:
    key_of = jax.random.split(jax.random.key(seed), 16)
    glu_value = draw_glu_value(jax.random.fold_in(key_of[15], 71), 0)
    glu_gate = scatter_about(key_of[1], (TOKENS, CONV), 1.5, 8.0, ((0, 16), (1, 2)))
    conv_kernel = scatter_about(key_of[2], (KERNEL, CONV), KERNEL ** -0.5, 1.0, ((1, 2),))
    conv_bias = scatter_about(key_of[3], (CONV,), 0.3, 1.5, ((0, 2),), jnp.float32)
    group_gain = jnp.clip(1.0 + 0.18 * jax.random.normal(key_of[4], (CONV,), jnp.float32), 0.1, 1.9)
    group_shift = scatter_about(key_of[5], (CONV,), 0.5, 2.5, ((0, 2),), jnp.float32)
    out_weight = scatter_about(key_of[6], (CONV, D), CONV ** -0.5, 0.1875)
    residual = draw_residual(jax.random.fold_in(key_of[15], 71), 0)
    ffn_gain = jnp.clip(1.0 + 0.18 * jax.random.normal(key_of[8], (D,), jnp.float32), 0.1, 1.9)
    expert_pick = draw_expert_pick(jax.random.fold_in(key_of[15], 71), 0)
    pair_logits = scatter_about(key_of[10], (TOKENS, 2), 0.3, 1.2, ((0, 32),), jnp.float32)
    group_prob = jnp.clip(jnp.exp(math.log(1.0) - 0.6931472 * jax.random.uniform(key_of[11], (TOKENS,), jnp.float32) ** block_scale(key_of[11], (TOKENS,), ((0, 32),), -0.2, 0.2)), 0.5, 1.0)
    gate_weight = scatter_about(key_of[12], (EXPERTS, D, FFE), D ** -0.5, 0.125, ((0, 32),))
    up_weight = scatter_about(key_of[13], (EXPERTS, D, FFE), D ** -0.5, 0.125, ((0, 32),))
    down_weight = scatter_about(key_of[14], (EXPERTS, FFE, D), (FFE // 8) ** -0.5, 0.75, ((0, 32),))
    return dict(glu_value=glu_value, glu_gate=glu_gate, conv_kernel=conv_kernel, conv_bias=conv_bias, group_gain=group_gain, group_shift=group_shift, out_weight=out_weight, residual=residual, ffn_gain=ffn_gain, expert_pick=expert_pick, pair_logits=pair_logits, group_prob=group_prob, gate_weight=gate_weight, up_weight=up_weight, down_weight=down_weight)


EPS = 1e-06

def conv_module(glu_value, glu_gate, conv_kernel, conv_bias, group_gain, group_shift):
    glued_rows = (glu_value.astype(jnp.float32) * jax.nn.sigmoid(glu_gate.astype(jnp.float32))).astype(jnp.bfloat16)
    reach_rows = conv_kernel.shape[0] - 1
    length = glued_rows.shape[0]
    padded = jnp.pad(glued_rows, ((reach_rows, 0), (0, 0))).astype(jnp.float32)
    kernel = conv_kernel.astype(jnp.float32)
    summed = jnp.zeros(glued_rows.shape, jnp.float32) + conv_bias.astype(jnp.float32)
    for offset in range(reach_rows + 1):
        summed = summed + kernel[offset] * padded[offset:offset + length]
    grouped = summed.reshape(length, CONV_GROUPS, -1)
    centre = lax.optimization_barrier(jnp.mean(grouped, axis=-1, keepdims=True))
    variance = lax.optimization_barrier(jnp.mean(jnp.square(grouped - centre), axis=-1, keepdims=True))
    leveled = ((grouped - centre) * lax.rsqrt(variance + EPS)).reshape(length, -1)
    return jax.nn.silu(leveled * group_gain + group_shift).astype(jnp.bfloat16)

def experts_apply(normed, expert_pick, gate_weight, up_weight, down_weight):
    picks = expert_pick.shape[1]
    slot_experts = expert_pick.reshape(-1)
    slot_total = slot_experts.shape[0]
    most_rows = N_SP * N_TP * CAP
    onehot = (slot_experts[:, None] == jnp.arange(EXPERTS, dtype=jnp.int32)[None, :]).astype(jnp.int32)
    before = (jnp.cumsum(onehot, axis=0) - onehot).astype(jnp.int32)
    slot_rank = lax.optimization_barrier(jnp.sum(before * onehot, axis=1)).astype(jnp.int32)
    slot_place = (slot_experts * most_rows + slot_rank).astype(jnp.int32)
    source_flat = jnp.full((EXPERTS * most_rows,), slot_total, jnp.int32)
    source_flat = source_flat.at[slot_place].set(jnp.arange(slot_total, dtype=jnp.int32))
    source_table = source_flat.reshape(EXPERTS, most_rows)
    padded_rows = jnp.concatenate([normed, jnp.zeros((1, normed.shape[1]), normed.dtype)], axis=0)

    def apply_expert(inputs):
        source_index, gate_part, up_part, down_part = inputs
        picked = padded_rows[source_index // picks]
        gate_out = jnp.dot(picked, gate_part, preferred_element_type=jnp.float32)
        up_out = jnp.dot(picked, up_part, preferred_element_type=jnp.float32)
        active = (jax.nn.silu(gate_out) * up_out).astype(jnp.bfloat16)
        return jnp.dot(active, down_part, preferred_element_type=jnp.float32).astype(jnp.bfloat16)
    answers = lax.map(apply_expert, (source_table, gate_weight, up_weight, down_weight))
    flat_answers = answers.reshape(EXPERTS * most_rows, -1)
    return flat_answers[slot_place].reshape(-1, picks, normed.shape[1])

def reference(glu_value, glu_gate, conv_kernel, conv_bias, group_gain, group_shift, out_weight, residual, ffn_gain, expert_pick, pair_logits, group_prob, gate_weight, up_weight, down_weight):
    mixed_rows = conv_module(glu_value, glu_gate, conv_kernel, conv_bias, group_gain, group_shift)
    projected = jnp.dot(mixed_rows, out_weight, preferred_element_type=jnp.float32)
    hidden = (residual.astype(jnp.float32) + projected).astype(jnp.bfloat16)
    hidden_full = hidden.astype(jnp.float32)
    scale_rows = lax.rsqrt(lax.optimization_barrier(jnp.mean(hidden_full * hidden_full, axis=-1, keepdims=True)) + EPS)
    normed = (hidden_full * scale_rows * ffn_gain).astype(jnp.bfloat16)
    answer = experts_apply(normed, expert_pick, gate_weight, up_weight, down_weight)
    first_share = group_prob * jax.nn.sigmoid(pair_logits[:, 0] - pair_logits[:, 1])
    second_share = group_prob * jax.nn.sigmoid(pair_logits[:, 1] - pair_logits[:, 0])
    combined = hidden_full + first_share[:, None] * answer[:, 0].astype(jnp.float32)
    combined = combined + second_share[:, None] * answer[:, 1].astype(jnp.float32)
    return combined.astype(jnp.bfloat16)
```

```python
import functools

import jax
import jax.numpy as jnp
from jax import lax
from jax.experimental import pallas as pl
from jax.experimental.pallas import tpu as pltpu
from jax.sharding import PartitionSpec as P

CONV_GROUPS = 8


EPS = 1e-06


PLANES = 4
MESH = pl.DeviceIdType.MESH
ORDER = (1, 3, 2)
ROWS_MIN = 16
HALVES = 2


def layer_kernel(
    cap,
    slot,
    value_hbm,
    glu_gate_hbm,
    taps_hbm,
    bias_hbm,
    gain_hbm,
    shift_hbm,
    residual_hbm,
    ffn_hbm,
    pick_hbm,
    logit_hbm,
    prob_hbm,
    out_hbm,
    gate_hbm,
    up_hbm,
    down_hbm,
    out_ref,
    value_ref,
    gate_ref,
    taps_ref,
    bias_ref,
    gain_ref,
    shift_ref,
    residual_ref,
    ffn_ref,
    pick_ref,
    logit_ref,
    prob_ref,
    isem,
    glued,
    hsend,
    hrecv,
    mixed,
    mrest,
    place_ref,
    meta_ref,
    normed_ref,
    hidden_ref,
    proj,
    out_v,
    zsend,
    zrecv,
    mrecv,
    xsend,
    xrecv,
    asend,
    arecv,
    csend,
    cret,
    gate_v,
    up_v,
    down_v,
    wsem,
    hss,
    hrs,
    tss,
    trs,
    zss,
    zrs,
    mss,
    mrs,
    xss,
    xrs,
    ass,
    ars,
    css,
    crs,
):
    n_tp = lax.axis_size("tp")
    chips = lax.axis_size("sp") // PLANES
    peers = chips * n_tp
    sp = lax.axis_index("sp")
    tp = lax.axis_index("tp")
    n_sp = lax.axis_size("sp")
    z = sp // chips
    here = sp % chips
    tokens = residual_ref.shape[0]
    length, channels = value_ref.shape
    reach = taps_ref.shape[0] - 1
    lead = hsend.shape[0]
    j = here * n_tp + tp
    slots = peers * slot
    group_rows = zsend.shape[2]
    half = zsend.shape[3]

    def span(h):
        return slice(h * half, (h + 1) * half)

    def plane(d):
        if d == 1:
            return z + 1 - 2 * (z % 2)
        if d == 2:
            return z + 2 - 4 * (z // 2)
        return PLANES - 1 - z

    def mate(d):
        return (plane(d) * chips + here, tp)

    def peer(k):
        return (z * chips + k // n_tp, k % n_tp)

    def zcopy(d, h):
        return pltpu.make_async_remote_copy(
            src_ref=zsend.at[d, h], dst_ref=zrecv.at[d, h],
            send_sem=zss.at[d, h], recv_sem=zrs.at[d, h],
            device_id=mate(d), device_id_type=MESH,
        )

    def mcopy(d):
        return pltpu.make_async_remote_copy(
            src_ref=meta_ref.at[d], dst_ref=mrecv.at[d], send_sem=mss.at[d], recv_sem=mrs.at[d],
            device_id=mate(d), device_id_type=MESH,
        )

    def ccopy(d, h):
        return pltpu.make_async_remote_copy(
            src_ref=csend.at[d, h], dst_ref=cret.at[d, h],
            send_sem=css.at[d, h], recv_sem=crs.at[d, h],
            device_id=mate(d), device_id_type=MESH,
        )

    def xcopy(d, h, o):
        rows = pl.ds(o * slot, slot)
        return pltpu.make_async_remote_copy(
            src_ref=xsend.at[d, h, rows], dst_ref=xrecv.at[d, h, rows],
            send_sem=xss.at[d, h, o], recv_sem=xrs.at[d, h, o],
            device_id=peer((j + o) % peers), device_id_type=MESH,
        )

    def acopy(d, h, o):
        rows = pl.ds(o * slot, slot)
        return pltpu.make_async_remote_copy(
            src_ref=asend.at[d, h, rows], dst_ref=arecv.at[d, h, rows],
            send_sem=ass.at[d, h, o], recv_sem=ars.at[d, h, o],
            device_id=peer((j + peers - o) % peers), device_id_type=MESH,
        )

    def halo():
        return pltpu.make_async_remote_copy(
            src_ref=hsend, dst_ref=hrecv, send_sem=hss.at[0], recv_sem=hrs.at[0],
            device_id=((sp + 1) % n_sp, tp), device_id_type=MESH,
        )

    block = 64

    def tcopy(o, begin, size):
        other = (tp + o) % n_tp
        rows = pl.ds(pl.multiple_of(other * tokens + begin, size), size)
        mark = begin // (block // 2)
        return pltpu.make_async_remote_copy(
            src_ref=mixed.at[rows], dst_ref=mrest.at[o, pl.ds(begin, size)],
            send_sem=tss.at[o, mark], recv_sem=trs.at[o, mark],
            device_id=(sp, other), device_id_type=MESH,
        )

    head_dev, tail_dev = sp == 0, sp == n_sp - 1
    barrier = pltpu.get_barrier_semaphore()
    for d in ORDER:
        pl.semaphore_signal(barrier, inc=1, device_id=mate(d), device_id_type=MESH)
    for o in range(1, peers):
        pl.semaphore_signal(
            barrier, inc=1, device_id=peer((j + o) % peers), device_id_type=MESH
        )

    @pl.when(jnp.logical_not(tail_dev))
    def _():
        pl.semaphore_signal(barrier, inc=1, device_id=(sp + 1, tp), device_id_type=MESH)

    @pl.when(jnp.logical_not(head_dev))
    def _():
        pl.semaphore_signal(barrier, inc=1, device_id=(sp - 1, tp), device_id_type=MESH)

    sources = (
        (value_hbm, value_ref), (glu_gate_hbm, gate_ref), (pick_hbm, pick_ref),
        (logit_hbm, logit_ref), (prob_hbm, prob_ref), (taps_hbm, taps_ref),
        (bias_hbm, bias_ref), (gain_hbm, gain_ref), (shift_hbm, shift_ref),
        (ffn_hbm, ffn_ref), (residual_hbm, residual_ref),
    )
    inputs = [pltpu.make_async_copy(a, b, isem.at[k]) for k, (a, b) in enumerate(sources)]
    for copy in inputs:
        copy.start()
    out_copy = pltpu.make_async_copy(out_hbm, out_v, wsem.at[3])
    weights = [
        pltpu.make_async_copy(gate_hbm.at[0], gate_v, wsem.at[0]),
        pltpu.make_async_copy(up_hbm.at[0], up_v, wsem.at[1]),
        pltpu.make_async_copy(down_hbm.at[0], down_v, wsem.at[2]),
    ]
    f32 = jnp.float32
    bf16 = jnp.bfloat16
    for copy in inputs[:2]:
        copy.wait()
    out_copy.start()
    for start in range(length - block, -1, -block):
        rows = slice(start, start + block)
        gated = value_ref[rows].astype(f32) / (1.0 + jnp.exp(-gate_ref[rows].astype(f32)))
        gated = gated.astype(bf16)
        glued[lead + start : lead + start + block] = gated.astype(f32)
        if start == length - block:
            hsend[...] = gated[block - lead :]
    for copy in inputs[2:5]:
        copy.wait()
    picks = pick_ref[...].astype(f32)
    logits = logit_ref[...]
    rows_of = [picks[0:1, :], picks[1:2, :], logits[0:1, :], logits[1:2, :]]
    sublane = lax.broadcasted_iota(jnp.int32, (128, tokens), 0)
    tall = jnp.zeros((128, tokens), f32)
    for k in range(2):
        tall = jnp.where(sublane == k, rows_of[k], tall)
    wide = tall.T
    cols = [wide[:, 0:1], wide[:, 1:2]]
    square = (tokens, tokens)
    earlier = lax.broadcasted_iota(jnp.int32, square, 0) < lax.broadcasted_iota(
        jnp.int32, square, 1
    )

    def group_of(pick):
        total = jnp.zeros(pick.shape, f32)
        for q in range(1, PLANES):
            total += jnp.where(pick >= (q * peers), 1.0, 0.0)
        return total

    def count(hit):
        return jnp.sum(jnp.where(hit & earlier, 1.0, 0.0), axis=0, keepdims=True)

    ranks = [count((cols[0] == r) | (cols[1] == r)) for r in rows_of[:2]]
    group_row = group_of(rows_of[0])
    spot = count(group_of(cols[0]) == group_row)
    away = group_row.astype(jnp.int32) ^ z
    at_row = away.astype(f32) * group_rows + spot
    row_id = lax.broadcasted_iota(jnp.int32, (PLANES * group_rows, tokens), 0).astype(f32)
    place_ref[...] = jnp.where(row_id == at_row, 1.0, 0.0).astype(bf16)
    gap = rows_of[2] - rows_of[3]
    shares = [prob_ref[...] / (1.0 + jnp.exp(-gap)), prob_ref[...] / (1.0 + jnp.exp(gap))]
    fields = [jnp.ones((1, tokens), f32)]
    for k in range(2):
        fields += [rows_of[k] - group_row * peers, ranks[k]]
    for share in shares:
        for _ in range(3):
            part = share.astype(bf16).astype(f32)
            fields.append(part)
            share = share - part
    field_id = lax.broadcasted_iota(jnp.int32, (16, tokens), 0)
    table = jnp.zeros((16, tokens), f32)
    for k, field in enumerate(fields):
        table = jnp.where(field_id == k, field, table)
    table = table.astype(bf16)
    meta_ref[...] = jnp.zeros(meta_ref.shape, f32)
    for d in range(PLANES):
        part = lax.dot_general(
            table,
            place_ref[d * group_rows : (d + 1) * group_rows, :],
            (((1,), (1,)), ((), ())),
            preferred_element_type=f32,
        )
        empty = (1.0 - part[0:1]) * 65536.0
        meta_ref[d, 0:1, :group_rows] = part[1:2] * slot + part[2:3] + empty
        meta_ref[d, 1:2, :group_rows] = part[3:4] * slot + part[4:5] + empty
        meta_ref[d, 2:3, :group_rows] = part[5:6] + part[6:7] + part[7:8]
        meta_ref[d, 3:4, :group_rows] = part[8:9] + part[9:10] + part[10:11]
    for copy in inputs[5:]:
        copy.wait()
    for copy in weights:
        copy.start()
    wide_group = channels * n_tp // CONV_GROUPS
    taps = taps_ref[...].astype(f32)
    spans = [(start, block) for start in range(length - block, 0, -block)]
    spans += [(block // 2, block // 2), (0, block // 2)]
    for start, size in spans:
        if start == length - block * 2:
            pl.semaphore_wait(
                barrier,
                len(ORDER) + peers - 1
                + jnp.where(head_dev, 0, 1) + jnp.where(tail_dev, 0, 1),
            )

            @pl.when(jnp.logical_not(tail_dev))
            def _():
                halo().start()

            for d in ORDER:
                mcopy(d).start()
        if start == 0:

            @pl.when(head_dev)
            def _():
                glued[:lead] = jnp.zeros((lead, channels), f32)

            @pl.when(jnp.logical_not(head_dev))
            def _():
                halo().wait_recv()
                glued[:lead] = hrecv[...].astype(f32)

        for low_lane in range(0, channels, wide_group):
            part = slice(low_lane, low_lane + wide_group)
            total = jnp.zeros((size, wide_group), f32) + bias_ref[:, part]
            for offset in range(reach + 1):
                first = start + lead - reach + offset
                total += taps[offset : offset + 1, part] * glued[first : first + size, part]
            centre = jnp.mean(total, axis=-1, keepdims=True)
            total = total - centre
            variance = jnp.mean(total * total, axis=-1, keepdims=True)
            level = total * lax.rsqrt(variance + EPS)
            level = level * gain_ref[:, part] + shift_ref[:, part]
            mixed[start : start + size, part] = (level / (1.0 + jnp.exp(-level))).astype(bf16)
        if start + size == length:
            continue
        pieces = (start,) if start + size + block < length else (start, start + size)
        for piece in pieces:
            for o in range(1, n_tp):

                @pl.when((tp + o) % n_tp == piece // tokens)
                def _():
                    tcopy(o, piece % tokens, size).start()

    out_copy.wait()

    def weight_rows(which):
        return out_v[pl.ds(pl.multiple_of(which * channels, channels), channels), :]

    own = mixed[pl.ds(pl.multiple_of(tp * tokens, tokens), tokens), :]
    proj[...] = jnp.dot(own, weight_rows(tp), preferred_element_type=f32)

    def arrivals(act):
        for who in range(n_tp):
            for start, size in spans:
                if start // tokens == who:
                    for o in range(1, n_tp):
                        act(who, o, start % tokens, size)

    def landed(who, o, begin, size):
        @pl.when(tp == who)
        def _():
            tcopy(o, begin, size).wait_recv()

    def left(who, o, begin, size):
        @pl.when((tp + o) % n_tp == who)
        def _():
            tcopy(o, begin, size).wait_send()

    arrivals(landed)
    for o in range(1, n_tp):
        proj[...] += jnp.dot(
            mrest[o], weight_rows((tp + n_tp - o) % n_tp), preferred_element_type=f32
        )
    for start in range(0, tokens, 16):
        rows = slice(start, start + 16)
        hidden = (residual_ref[rows].astype(f32) + proj[rows]).astype(bf16)
        hidden_ref[rows] = hidden
        full = hidden.astype(f32)
        scale = lax.rsqrt(jnp.mean(full * full, axis=-1, keepdims=True) + EPS)
        normed_ref[rows] = (full * scale * ffn_ref[...]).astype(bf16)

    inner = (z >= 1) & (z < PLANES - 1)
    for d in ORDER + (0,):
        for h in range(HALVES):
            picked = jnp.dot(
                place_ref[d * group_rows : (d + 1) * group_rows, :],
                normed_ref[:, span(h)],
                preferred_element_type=f32,
            )
            zsend[d, h] = picked.astype(bf16)
            if d == 1:
                zcopy(d, h).start()
            elif d:

                @pl.when(inner)
                def _():
                    zcopy(d, h).start()


    def places(d):
        meta = meta_ref[0] if d == 0 else mrecv[d]
        row = lax.broadcasted_iota(jnp.int32, (slots, group_rows), 0).astype(jnp.float32)
        shift = (j * slot).astype(jnp.float32)
        out = []
        for k in range(2):
            at = meta[k : k + 1, :group_rows] - shift
            at = jnp.where(at < 0, at + slots, at)
            out.append(row == at)
        shares = [meta[2 + k : 3 + k, :group_rows] for k in range(2)]
        return out, shares

    def entry(d):
        if d:
            mcopy(d).wait_recv()
        at, _ = places(d)
        chosen = jnp.where(at[0] | at[1], 1.0, 0.0).astype(jnp.bfloat16)
        for h in range(HALVES):
            if d:
                zcopy(d, h).wait_recv()
            rows = zsend[0, h] if d == 0 else zrecv[d, h]
            spread = jnp.dot(chosen, rows, preferred_element_type=jnp.float32)
            spread = spread.astype(jnp.bfloat16)
            xrecv[d, h, :slot] = spread[:slot]
            xsend[d, h, slot:] = spread[slot:]
            for o in range(1, peers):
                xcopy(d, h, o).start()

    def expert(d):
        gate_out = None
        for h in range(HALVES):
            for o in range(1, peers):
                xcopy(d, h, o).wait_recv()
            rows = xrecv[d, h]
            gate_part = jnp.dot(rows, gate_v[span(h), :], preferred_element_type=jnp.float32)
            up_part = jnp.dot(rows, up_v[span(h), :], preferred_element_type=jnp.float32)
            gate_out = gate_part if h == 0 else gate_out + gate_part
            up_out = up_part if h == 0 else up_out + up_part
        active = (gate_out / (1.0 + jnp.exp(-gate_out)) * up_out).astype(jnp.bfloat16)
        for h in range(HALVES):
            answer = jnp.dot(active, down_v[:, span(h)], preferred_element_type=jnp.float32)
            answer = answer.astype(jnp.bfloat16)
            arecv[d, h, :slot] = answer[:slot]
            asend[d, h, slot:] = answer[slot:]

    def reply(d, halves=tuple(range(HALVES))):
        for h in halves:
            for o in range(1, peers):
                acopy(d, h, o).start()

    def combine(d, halves=tuple(range(HALVES))):
        at, shares = places(d)
        mix = jnp.where(at[0], shares[0], 0.0) + jnp.where(at[1], shares[1], 0.0)
        high = mix.astype(jnp.bfloat16)
        low = (mix - high.astype(jnp.float32)).astype(jnp.bfloat16)
        dims = (((0,), (0,)), ((), ()))
        for h in halves:
            for o in range(1, peers):
                acopy(d, h, o).wait_recv()
            answers = arecv[d, h]
            total = lax.dot_general(high, answers, dims, preferred_element_type=jnp.float32)
            total += lax.dot_general(low, answers, dims, preferred_element_type=jnp.float32)
            if d == 0:
                cret[0, h] = total.astype(jnp.bfloat16)
            else:
                csend[d, h] = total.astype(jnp.bfloat16)
                ccopy(d, h).start()

    head, rest = (0,), tuple(range(1, HALVES))
    entry(0)

    @pl.when(inner)
    def _():
        entry(3)
        entry(1)
        for copy in weights:
            copy.wait()
        expert(0)
        expert(3)
        reply(3)
        expert(1)
        entry(2)
        reply(1, head)
        combine(3)
        expert(2)
        reply(2)
        reply(1, rest)
        combine(1, head)
        combine(2, head)
        reply(0)
        combine(2, rest)
        combine(1, rest)
        combine(0)

    @pl.when(jnp.logical_not(inner))
    def _():
        entry(1)
        for copy in weights:
            copy.wait()
        expert(0)
        for d in (2, 3):
            for h in range(HALVES):
                zcopy(d, h).start()
        entry(2)
        expert(1)
        reply(1, head)
        expert(2)
        reply(2)
        entry(3)
        reply(1, rest)
        combine(2)
        combine(1, head)
        expert(3)
        reply(3)
        combine(1, rest)
        reply(0)
        combine(3)
        combine(0)

    dims = (((0,), (0,)), ((), ()))
    for h in range(HALVES):
        total = hidden_ref[:, span(h)].astype(jnp.float32)
        for d in (2, 1, 3, 0):
            if d:
                ccopy(d, h).wait_recv()
            total += lax.dot_general(
                place_ref[d * group_rows : (d + 1) * group_rows, :],
                cret[d, h],
                dims,
                preferred_element_type=jnp.float32,
            )
        out_ref[:, span(h)] = total.astype(jnp.bfloat16)

    @pl.when(jnp.logical_not(tail_dev))
    def _():
        halo().wait_send()

    arrivals(left)
    for d in ORDER:
        mcopy(d).wait_send()
        for h in range(HALVES):
            zcopy(d, h).wait_send()
            ccopy(d, h).wait_send()
    for d in range(PLANES):
        for h in range(HALVES):
            for o in range(1, peers):
                xcopy(d, h, o).wait_send()
                acopy(d, h, o).wait_send()


def local(
    glu_value,
    glu_gate,
    conv_kernel,
    conv_bias,
    group_gain,
    group_shift,
    out_weight,
    residual,
    ffn_gain,
    expert_pick,
    pair_logits,
    group_prob,
    gate_weight,
    up_weight,
    down_weight,
):
    rows, width = residual.shape
    length, channels = glu_value.shape
    n_tp = lax.axis_size("tp")
    experts_all = lax.axis_size("sp") * n_tp
    cap = 4 * rows // experts_all
    peers = experts_all // PLANES
    group_rows = peers * cap // 2
    slot = max(cap, ROWS_MIN)
    slots = peers * slot
    lead = -(-(conv_kernel.shape[0] - 1) // 16) * 16
    bf16 = jnp.bfloat16
    f32 = jnp.float32
    vmem = pl.BlockSpec(memory_space=pltpu.VMEM)
    hbm = pl.BlockSpec(memory_space=pl.ANY)
    dma = pltpu.SemaphoreType.DMA
    return pl.pallas_call(
        functools.partial(layer_kernel, cap, slot),
        out_shape=pltpu.VMEM((rows, width), bf16),
        in_specs=[hbm] * 15,
        out_specs=vmem,
        scratch_shapes=[
            pltpu.VMEM(glu_value.shape, bf16),
            pltpu.VMEM(glu_gate.shape, bf16),
            pltpu.VMEM(conv_kernel.shape, bf16),
            pltpu.VMEM((1, channels), f32),
            pltpu.VMEM((1, channels), f32),
            pltpu.VMEM((1, channels), f32),
            pltpu.VMEM((rows, width), bf16),
            pltpu.VMEM((1, width), f32),
            pltpu.VMEM((2, rows), jnp.int32),
            pltpu.VMEM((2, rows), f32),
            pltpu.VMEM((1, rows), f32),
            dma((11,)),
            pltpu.VMEM((lead + length, channels), f32),
            pltpu.VMEM((lead, channels), bf16),
            pltpu.VMEM((lead, channels), bf16),
            pltpu.VMEM((length, channels), bf16),
            pltpu.VMEM((n_tp, rows, channels), bf16),
            pltpu.VMEM((PLANES * group_rows, rows), bf16),
            pltpu.VMEM((PLANES, 8, 128), f32),
            pltpu.VMEM((rows, width), bf16),
            pltpu.VMEM((rows, width), bf16),
            pltpu.VMEM((rows, width), f32),
            pltpu.VMEM(out_weight.shape, bf16),
            pltpu.VMEM((PLANES, HALVES, group_rows, width // HALVES), bf16),
            pltpu.VMEM((PLANES, HALVES, group_rows, width // HALVES), bf16),
            pltpu.VMEM((PLANES, 8, 128), f32),
            pltpu.VMEM((PLANES, HALVES, slots, width // HALVES), bf16),
            pltpu.VMEM((PLANES, HALVES, slots, width // HALVES), bf16),
            pltpu.VMEM((PLANES, HALVES, slots, width // HALVES), bf16),
            pltpu.VMEM((PLANES, HALVES, slots, width // HALVES), bf16),
            pltpu.VMEM((PLANES, HALVES, group_rows, width // HALVES), bf16),
            pltpu.VMEM((PLANES, HALVES, group_rows, width // HALVES), bf16),
            pltpu.VMEM(gate_weight.shape[1:], bf16),
            pltpu.VMEM(up_weight.shape[1:], bf16),
            pltpu.VMEM(down_weight.shape[1:], bf16),
            dma((4,)),
            dma((1,)),
            dma((1,)),
            dma((n_tp, rows // 32)),
            dma((n_tp, rows // 32)),
            dma((PLANES, HALVES)),
            dma((PLANES, HALVES)),
            dma((PLANES,)),
            dma((PLANES,)),
            dma((PLANES, HALVES, peers)),
            dma((PLANES, HALVES, peers)),
            dma((PLANES, HALVES, peers)),
            dma((PLANES, HALVES, peers)),
            dma((PLANES, HALVES)),
            dma((PLANES, HALVES)),
        ],
        compiler_params=pltpu.CompilerParams(
            collective_id=0, has_side_effects=True, vmem_limit_bytes=62 * 1024 * 1024
        ),
    )(
        glu_value,
        glu_gate,
        conv_kernel,
        conv_bias[None, :],
        group_gain[None, :],
        group_shift[None, :],
        residual,
        ffn_gain[None, :],
        expert_pick.T,
        pair_logits.T,
        group_prob[None, :],
        out_weight,
        gate_weight,
        up_weight,
        down_weight,
    )


def solution(mesh):
    in_specs = (
        P("sp", "tp"),
        P("sp", "tp"),
        P(None, "tp"),
        P("tp"),
        P("tp"),
        P("tp"),
        P(),
        P(("sp", "tp"), None),
        P(),
        P(("sp", "tp"), None),
        P(("sp", "tp"), None),
        P(("sp", "tp")),
        P(("sp", "tp"), None, None),
        P(("sp", "tp"), None, None),
        P(("sp", "tp"), None, None),
    )
    out_specs = P(("sp", "tp"), None)
    return jax.shard_map(local, mesh=mesh, in_specs=in_specs, out_specs=out_specs, check_vma=False)
```

```python
import functools

import jax
import jax.numpy as jnp
from jax import lax
from jax.experimental import pallas as pl
from jax.experimental.pallas import tpu as pltpu
from jax.sharding import PartitionSpec as P

CONV_GROUPS = 8


EPS = 1e-06


PLANES = 4
MESH = pl.DeviceIdType.MESH
ORDER = (1, 3, 2)
ROWS_MIN = 16
HALVES = 2


def layer_kernel(
    cap,
    slot,
    value_hbm,
    glu_gate_hbm,
    taps_hbm,
    bias_hbm,
    gain_hbm,
    shift_hbm,
    residual_hbm,
    ffn_hbm,
    pick_hbm,
    logit_hbm,
    prob_hbm,
    out_hbm,
    gate_hbm,
    up_hbm,
    down_hbm,
    out_ref,
    value_ref,
    gate_ref,
    taps_ref,
    bias_ref,
    gain_ref,
    shift_ref,
    residual_ref,
    ffn_ref,
    pick_ref,
    logit_ref,
    prob_ref,
    isem,
    glued,
    hsend,
    hrecv,
    mixed,
    mrest,
    place_ref,
    meta_ref,
    normed_ref,
    hidden_ref,
    proj,
    out_v,
    zsend,
    zrecv,
    mrecv,
    xsend,
    xrecv,
    asend,
    arecv,
    csend,
    cret,
    gate_v,
    up_v,
    down_v,
    wsem,
    hss,
    hrs,
    tss,
    trs,
    zss,
    zrs,
    mss,
    mrs,
    xss,
    xrs,
    ass,
    ars,
    css,
    crs,
):
    n_tp = lax.axis_size("tp")
    chips = lax.axis_size("sp") // PLANES
    peers = chips * n_tp
    sp = lax.axis_index("sp")
    tp = lax.axis_index("tp")
    n_sp = lax.axis_size("sp")
    z = sp // chips
    here = sp % chips
    tokens = residual_ref.shape[0]
    length, channels = value_ref.shape
    reach = taps_ref.shape[0] - 1
    lead = hsend.shape[0]
    j = here * n_tp + tp
    slots = peers * slot
    group_rows = zsend.shape[2]
    half = zsend.shape[3]

    def span(h):
        return slice(h * half, (h + 1) * half)

    def plane(d):
        if d == 1:
            return z + 1 - 2 * (z % 2)
        if d == 2:
            return z + 2 - 4 * (z // 2)
        return PLANES - 1 - z

    def mate(d):
        return (plane(d) * chips + here, tp)

    def peer(k):
        return (z * chips + k // n_tp, k % n_tp)

    def zcopy(d, h):
        return pltpu.make_async_remote_copy(
            src_ref=zsend.at[d, h], dst_ref=zrecv.at[d, h],
            send_sem=zss.at[d, h], recv_sem=zrs.at[d, h],
            device_id=mate(d), device_id_type=MESH,
        )

    def mcopy(d):
        return pltpu.make_async_remote_copy(
            src_ref=meta_ref.at[d], dst_ref=mrecv.at[d], send_sem=mss.at[d], recv_sem=mrs.at[d],
            device_id=mate(d), device_id_type=MESH,
        )

    def ccopy(d, h):
        return pltpu.make_async_remote_copy(
            src_ref=csend.at[d, h], dst_ref=cret.at[d, h],
            send_sem=css.at[d, h], recv_sem=crs.at[d, h],
            device_id=mate(d), device_id_type=MESH,
        )

    def xcopy(d, h, o):
        rows = pl.ds(o * slot, slot)
        return pltpu.make_async_remote_copy(
            src_ref=xsend.at[d, h, rows], dst_ref=xrecv.at[d, h, rows],
            send_sem=xss.at[d, h, o], recv_sem=xrs.at[d, h, o],
            device_id=peer((j + o) % peers), device_id_type=MESH,
        )

    def acopy(d, h, o):
        rows = pl.ds(o * slot, slot)
        return pltpu.make_async_remote_copy(
            src_ref=asend.at[d, h, rows], dst_ref=arecv.at[d, h, rows],
            send_sem=ass.at[d, h, o], recv_sem=ars.at[d, h, o],
            device_id=peer((j + peers - o) % peers), device_id_type=MESH,
        )

    def halo():
        return pltpu.make_async_remote_copy(
            src_ref=hsend, dst_ref=hrecv, send_sem=hss.at[0], recv_sem=hrs.at[0],
            device_id=((sp + 1) % n_sp, tp), device_id_type=MESH,
        )

    block = 64

    def tcopy(o, begin, size):
        other = (tp + o) % n_tp
        rows = pl.ds(pl.multiple_of(other * tokens + begin, size), size)
        mark = begin // (block // 2)
        return pltpu.make_async_remote_copy(
            src_ref=mixed.at[rows], dst_ref=mrest.at[o, pl.ds(begin, size)],
            send_sem=tss.at[o, mark], recv_sem=trs.at[o, mark],
            device_id=(sp, other), device_id_type=MESH,
        )

    head_dev, tail_dev = sp == 0, sp == n_sp - 1
    barrier = pltpu.get_barrier_semaphore()
    for d in ORDER:
        pl.semaphore_signal(barrier, inc=1, device_id=mate(d), device_id_type=MESH)
    for o in range(1, peers):
        pl.semaphore_signal(
            barrier, inc=1, device_id=peer((j + o) % peers), device_id_type=MESH
        )

    @pl.when(jnp.logical_not(tail_dev))
    def _():
        pl.semaphore_signal(barrier, inc=1, device_id=(sp + 1, tp), device_id_type=MESH)

    @pl.when(jnp.logical_not(head_dev))
    def _():
        pl.semaphore_signal(barrier, inc=1, device_id=(sp - 1, tp), device_id_type=MESH)

    sources = (
        (value_hbm, value_ref), (glu_gate_hbm, gate_ref), (pick_hbm, pick_ref),
        (logit_hbm, logit_ref), (prob_hbm, prob_ref), (taps_hbm, taps_ref),
        (bias_hbm, bias_ref), (gain_hbm, gain_ref), (shift_hbm, shift_ref),
        (ffn_hbm, ffn_ref), (residual_hbm, residual_ref),
    )
    inputs = [pltpu.make_async_copy(a, b, isem.at[k]) for k, (a, b) in enumerate(sources)]
    for copy in inputs:
        copy.start()
    out_copy = pltpu.make_async_copy(out_hbm, out_v, wsem.at[3])
    weights = [
        pltpu.make_async_copy(gate_hbm.at[0], gate_v, wsem.at[0]),
        pltpu.make_async_copy(up_hbm.at[0], up_v, wsem.at[1]),
        pltpu.make_async_copy(down_hbm.at[0], down_v, wsem.at[2]),
    ]
    f32 = jnp.float32
    bf16 = jnp.bfloat16
    for copy in inputs[:2]:
        copy.wait()
    out_copy.start()
    for start in range(length - block, -1, -block):
        rows = slice(start, start + block)
        gated = value_ref[rows].astype(f32) / (1.0 + jnp.exp(-gate_ref[rows].astype(f32)))
        gated = gated.astype(bf16)
        glued[lead + start : lead + start + block] = gated.astype(f32)
        if start == length - block:
            hsend[...] = gated[block - lead :]
    for copy in inputs[2:5]:
        copy.wait()
    picks = pick_ref[...].astype(f32)
    logits = logit_ref[...]
    rows_of = [picks[0:1, :], picks[1:2, :], logits[0:1, :], logits[1:2, :]]
    sublane = lax.broadcasted_iota(jnp.int32, (128, tokens), 0)
    tall = jnp.zeros((128, tokens), f32)
    for k in range(2):
        tall = jnp.where(sublane == k, rows_of[k], tall)
    wide = tall.T
    cols = [wide[:, 0:1], wide[:, 1:2]]
    square = (tokens, tokens)
    earlier = lax.broadcasted_iota(jnp.int32, square, 0) < lax.broadcasted_iota(
        jnp.int32, square, 1
    )

    def group_of(pick):
        total = jnp.zeros(pick.shape, f32)
        for q in range(1, PLANES):
            total += jnp.where(pick >= (q * peers), 1.0, 0.0)
        return total

    def count(hit):
        return jnp.sum(jnp.where(hit & earlier, 1.0, 0.0), axis=0, keepdims=True)

    ranks = [count((cols[0] == r) | (cols[1] == r)) for r in rows_of[:2]]
    group_row = group_of(rows_of[0])
    spot = count(group_of(cols[0]) == group_row)
    away = group_row.astype(jnp.int32) ^ z
    at_row = away.astype(f32) * group_rows + spot
    row_id = lax.broadcasted_iota(jnp.int32, (PLANES * group_rows, tokens), 0).astype(f32)
    place_ref[...] = jnp.where(row_id == at_row, 1.0, 0.0).astype(bf16)
    gap = rows_of[2] - rows_of[3]
    shares = [prob_ref[...] / (1.0 + jnp.exp(-gap)), prob_ref[...] / (1.0 + jnp.exp(gap))]
    fields = [jnp.ones((1, tokens), f32)]
    for k in range(2):
        fields += [rows_of[k] - group_row * peers, ranks[k]]
    for share in shares:
        for _ in range(3):
            part = share.astype(bf16).astype(f32)
            fields.append(part)
            share = share - part
    field_id = lax.broadcasted_iota(jnp.int32, (16, tokens), 0)
    table = jnp.zeros((16, tokens), f32)
    for k, field in enumerate(fields):
        table = jnp.where(field_id == k, field, table)
    table = table.astype(bf16)
    meta_ref[...] = jnp.zeros(meta_ref.shape, f32)
    for d in range(PLANES):
        part = lax.dot_general(
            table,
            place_ref[d * group_rows : (d + 1) * group_rows, :],
            (((1,), (1,)), ((), ())),
            preferred_element_type=f32,
        )
        empty = (1.0 - part[0:1]) * 65536.0
        meta_ref[d, 0:1, :group_rows] = part[1:2] * slot + part[2:3] + empty
        meta_ref[d, 1:2, :group_rows] = part[3:4] * slot + part[4:5] + empty
        meta_ref[d, 2:3, :group_rows] = part[5:6] + part[6:7] + part[7:8]
        meta_ref[d, 3:4, :group_rows] = part[8:9] + part[9:10] + part[10:11]
    for copy in inputs[5:]:
        copy.wait()
    for copy in weights:
        copy.start()
    wide_group = channels * n_tp // CONV_GROUPS
    taps = taps_ref[...].astype(f32)
    def enter():
        pl.semaphore_wait(
            barrier,
            len(ORDER) + peers - 1
            + jnp.where(head_dev, 0, 1) + jnp.where(tail_dev, 0, 1),
        )

        @pl.when(jnp.logical_not(tail_dev))
        def _():
            halo().start()

        for d in ORDER:
            mcopy(d).start()

    @pl.when(z > 0)
    def _():
        enter()

    spans = [(start, block) for start in range(length - block, 0, -block)]
    spans += [(block // 2, block // 2), (0, block // 2)]
    for start, size in spans:
        if start == length - block * 2:

            @pl.when(z == 0)
            def _():
                enter()

        if start == 0:

            @pl.when(head_dev)
            def _():
                glued[:lead] = jnp.zeros((lead, channels), f32)

            @pl.when(jnp.logical_not(head_dev))
            def _():
                halo().wait_recv()
                glued[:lead] = hrecv[...].astype(f32)

        for low_lane in range(0, channels, wide_group):
            part = slice(low_lane, low_lane + wide_group)
            total = jnp.zeros((size, wide_group), f32) + bias_ref[:, part]
            for offset in range(reach + 1):
                first = start + lead - reach + offset
                total += taps[offset : offset + 1, part] * glued[first : first + size, part]
            centre = jnp.mean(total, axis=-1, keepdims=True)
            total = total - centre
            variance = jnp.mean(total * total, axis=-1, keepdims=True)
            level = total * lax.rsqrt(variance + EPS)
            level = level * gain_ref[:, part] + shift_ref[:, part]
            mixed[start : start + size, part] = (level / (1.0 + jnp.exp(-level))).astype(bf16)
        if start + size == length:
            continue
        pieces = (start,) if start + size + block < length else (start, start + size)
        for piece in pieces:
            for o in range(1, n_tp):

                @pl.when((tp + o) % n_tp == piece // tokens)
                def _():
                    tcopy(o, piece % tokens, size).start()

    out_copy.wait()

    def weight_rows(which):
        return out_v[pl.ds(pl.multiple_of(which * channels, channels), channels), :]

    own = mixed[pl.ds(pl.multiple_of(tp * tokens, tokens), tokens), :]
    proj[...] = jnp.dot(own, weight_rows(tp), preferred_element_type=f32)

    def arrivals(act):
        for who in range(n_tp):
            for start, size in spans:
                if start // tokens == who:
                    for o in range(1, n_tp):
                        act(who, o, start % tokens, size)

    def landed(who, o, begin, size):
        @pl.when(tp == who)
        def _():
            tcopy(o, begin, size).wait_recv()

    def left(who, o, begin, size):
        @pl.when((tp + o) % n_tp == who)
        def _():
            tcopy(o, begin, size).wait_send()

    arrivals(landed)
    for o in range(1, n_tp):
        proj[...] += jnp.dot(
            mrest[o], weight_rows((tp + n_tp - o) % n_tp), preferred_element_type=f32
        )
    for start in range(0, tokens, 16):
        rows = slice(start, start + 16)
        hidden = (residual_ref[rows].astype(f32) + proj[rows]).astype(bf16)
        hidden_ref[rows] = hidden
        full = hidden.astype(f32)
        scale = lax.rsqrt(jnp.mean(full * full, axis=-1, keepdims=True) + EPS)
        normed_ref[rows] = (full * scale * ffn_ref[...]).astype(bf16)

    inner = (z >= 1) & (z < PLANES - 1)
    for d in ORDER + (0,):
        for h in range(HALVES):
            picked = jnp.dot(
                place_ref[d * group_rows : (d + 1) * group_rows, :],
                normed_ref[:, span(h)],
                preferred_element_type=f32,
            )
            zsend[d, h] = picked.astype(bf16)
            if d == 1:
                zcopy(d, h).start()
            elif d:

                @pl.when(inner)
                def _():
                    zcopy(d, h).start()


    def places(d):
        meta = meta_ref[0] if d == 0 else mrecv[d]
        row = lax.broadcasted_iota(jnp.int32, (slots, group_rows), 0).astype(jnp.float32)
        shift = (j * slot).astype(jnp.float32)
        out = []
        for k in range(2):
            at = meta[k : k + 1, :group_rows] - shift
            at = jnp.where(at < 0, at + slots, at)
            out.append(row == at)
        shares = [meta[2 + k : 3 + k, :group_rows] for k in range(2)]
        return out, shares

    def entry(d, after=()):
        if d:
            mcopy(d).wait_recv()
        at, _ = places(d)
        chosen = jnp.where(at[0] | at[1], 1.0, 0.0).astype(jnp.bfloat16)
        for h in range(HALVES):
            if d:
                zcopy(d, h).wait_recv()
            for who in range(n_tp if after else 0):
                if h == min(who, HALVES - 1):

                    @pl.when(tp == who)
                    def _():
                        for later in after:
                            for k in range(HALVES):
                                zcopy(later, k).start()

            rows = zsend[0, h] if d == 0 else zrecv[d, h]
            spread = jnp.dot(chosen, rows, preferred_element_type=jnp.float32)
            spread = spread.astype(jnp.bfloat16)
            xrecv[d, h, :slot] = spread[:slot]
            xsend[d, h, slot:] = spread[slot:]
            for o in range(1, peers):
                xcopy(d, h, o).start()

    def expert(d):
        gate_out = None
        for h in range(HALVES):
            for o in range(1, peers):
                xcopy(d, h, o).wait_recv()
            rows = xrecv[d, h]
            gate_part = jnp.dot(rows, gate_v[span(h), :], preferred_element_type=jnp.float32)
            up_part = jnp.dot(rows, up_v[span(h), :], preferred_element_type=jnp.float32)
            gate_out = gate_part if h == 0 else gate_out + gate_part
            up_out = up_part if h == 0 else up_out + up_part
        active = (gate_out / (1.0 + jnp.exp(-gate_out)) * up_out).astype(jnp.bfloat16)
        for h in range(HALVES):
            answer = jnp.dot(active, down_v[:, span(h)], preferred_element_type=jnp.float32)
            answer = answer.astype(jnp.bfloat16)
            arecv[d, h, :slot] = answer[:slot]
            asend[d, h, slot:] = answer[slot:]

    def reply(d, halves=tuple(range(HALVES))):
        for h in halves:
            for o in range(1, peers):
                acopy(d, h, o).start()

    def combine(d, halves=tuple(range(HALVES))):
        at, shares = places(d)
        mix = jnp.where(at[0], shares[0], 0.0) + jnp.where(at[1], shares[1], 0.0)
        high = mix.astype(jnp.bfloat16)
        low = (mix - high.astype(jnp.float32)).astype(jnp.bfloat16)
        dims = (((0,), (0,)), ((), ()))
        for h in halves:
            for o in range(1, peers):
                acopy(d, h, o).wait_recv()
            answers = arecv[d, h]
            total = lax.dot_general(high, answers, dims, preferred_element_type=jnp.float32)
            total += lax.dot_general(low, answers, dims, preferred_element_type=jnp.float32)
            if d == 0:
                cret[0, h] = total.astype(jnp.bfloat16)
            else:
                csend[d, h] = total.astype(jnp.bfloat16)
                ccopy(d, h).start()

    head, rest = (0,), tuple(range(1, HALVES))
    entry(0)

    @pl.when(inner)
    def _():
        entry(3)
        entry(1)
        for copy in weights:
            copy.wait()
        expert(0)
        expert(3)
        reply(3)
        expert(1)
        reply(1, head)
        combine(3)
        entry(2)
        reply(1, rest)
        combine(1, head)
        expert(2)
        reply(2)
        combine(1, rest)
        reply(0)
        combine(2)
        combine(0)

    @pl.when(jnp.logical_not(inner))
    def _():
        entry(1)
        for copy in weights:
            copy.wait()
        expert(0)
        entry(2, after=(3, 2))
        expert(1)
        entry(3)
        expert(2)
        reply(2)
        expert(3)
        reply(3)
        combine(2)
        reply(1)
        combine(3)
        reply(0)
        combine(1)
        combine(0)

    dims = (((0,), (0,)), ((), ()))
    for h in range(HALVES):
        total = hidden_ref[:, span(h)].astype(jnp.float32)
        for d in (2, 1, 3, 0):
            if d:
                ccopy(d, h).wait_recv()
            total += lax.dot_general(
                place_ref[d * group_rows : (d + 1) * group_rows, :],
                cret[d, h],
                dims,
                preferred_element_type=jnp.float32,
            )
        out_ref[:, span(h)] = total.astype(jnp.bfloat16)

    @pl.when(jnp.logical_not(tail_dev))
    def _():
        halo().wait_send()

    arrivals(left)
    for d in ORDER:
        mcopy(d).wait_send()
        for h in range(HALVES):
            zcopy(d, h).wait_send()
            ccopy(d, h).wait_send()
    for d in range(PLANES):
        for h in range(HALVES):
            for o in range(1, peers):
                xcopy(d, h, o).wait_send()
                acopy(d, h, o).wait_send()


def local(
    glu_value,
    glu_gate,
    conv_kernel,
    conv_bias,
    group_gain,
    group_shift,
    out_weight,
    residual,
    ffn_gain,
    expert_pick,
    pair_logits,
    group_prob,
    gate_weight,
    up_weight,
    down_weight,
):
    rows, width = residual.shape
    length, channels = glu_value.shape
    n_tp = lax.axis_size("tp")
    experts_all = lax.axis_size("sp") * n_tp
    cap = 4 * rows // experts_all
    peers = experts_all // PLANES
    group_rows = peers * cap // 2
    slot = max(cap, ROWS_MIN)
    slots = peers * slot
    lead = -(-(conv_kernel.shape[0] - 1) // 16) * 16
    bf16 = jnp.bfloat16
    f32 = jnp.float32
    vmem = pl.BlockSpec(memory_space=pltpu.VMEM)
    hbm = pl.BlockSpec(memory_space=pl.ANY)
    dma = pltpu.SemaphoreType.DMA
    return pl.pallas_call(
        functools.partial(layer_kernel, cap, slot),
        out_shape=pltpu.VMEM((rows, width), bf16),
        in_specs=[hbm] * 15,
        out_specs=vmem,
        scratch_shapes=[
            pltpu.VMEM(glu_value.shape, bf16),
            pltpu.VMEM(glu_gate.shape, bf16),
            pltpu.VMEM(conv_kernel.shape, bf16),
            pltpu.VMEM((1, channels), f32),
            pltpu.VMEM((1, channels), f32),
            pltpu.VMEM((1, channels), f32),
            pltpu.VMEM((rows, width), bf16),
            pltpu.VMEM((1, width), f32),
            pltpu.VMEM((2, rows), jnp.int32),
            pltpu.VMEM((2, rows), f32),
            pltpu.VMEM((1, rows), f32),
            dma((11,)),
            pltpu.VMEM((lead + length, channels), f32),
            pltpu.VMEM((lead, channels), bf16),
            pltpu.VMEM((lead, channels), bf16),
            pltpu.VMEM((length, channels), bf16),
            pltpu.VMEM((n_tp, rows, channels), bf16),
            pltpu.VMEM((PLANES * group_rows, rows), bf16),
            pltpu.VMEM((PLANES, 8, 128), f32),
            pltpu.VMEM((rows, width), bf16),
            pltpu.VMEM((rows, width), bf16),
            pltpu.VMEM((rows, width), f32),
            pltpu.VMEM(out_weight.shape, bf16),
            pltpu.VMEM((PLANES, HALVES, group_rows, width // HALVES), bf16),
            pltpu.VMEM((PLANES, HALVES, group_rows, width // HALVES), bf16),
            pltpu.VMEM((PLANES, 8, 128), f32),
            pltpu.VMEM((PLANES, HALVES, slots, width // HALVES), bf16),
            pltpu.VMEM((PLANES, HALVES, slots, width // HALVES), bf16),
            pltpu.VMEM((PLANES, HALVES, slots, width // HALVES), bf16),
            pltpu.VMEM((PLANES, HALVES, slots, width // HALVES), bf16),
            pltpu.VMEM((PLANES, HALVES, group_rows, width // HALVES), bf16),
            pltpu.VMEM((PLANES, HALVES, group_rows, width // HALVES), bf16),
            pltpu.VMEM(gate_weight.shape[1:], bf16),
            pltpu.VMEM(up_weight.shape[1:], bf16),
            pltpu.VMEM(down_weight.shape[1:], bf16),
            dma((4,)),
            dma((1,)),
            dma((1,)),
            dma((n_tp, rows // 32)),
            dma((n_tp, rows // 32)),
            dma((PLANES, HALVES)),
            dma((PLANES, HALVES)),
            dma((PLANES,)),
            dma((PLANES,)),
            dma((PLANES, HALVES, peers)),
            dma((PLANES, HALVES, peers)),
            dma((PLANES, HALVES, peers)),
            dma((PLANES, HALVES, peers)),
            dma((PLANES, HALVES)),
            dma((PLANES, HALVES)),
        ],
        compiler_params=pltpu.CompilerParams(
            collective_id=0, has_side_effects=True, vmem_limit_bytes=62 * 1024 * 1024
        ),
    )(
        glu_value,
        glu_gate,
        conv_kernel,
        conv_bias[None, :],
        group_gain[None, :],
        group_shift[None, :],
        residual,
        ffn_gain[None, :],
        expert_pick.T,
        pair_logits.T,
        group_prob[None, :],
        out_weight,
        gate_weight,
        up_weight,
        down_weight,
    )


def solution(mesh):
    in_specs = (
        P("sp", "tp"),
        P("sp", "tp"),
        P(None, "tp"),
        P("tp"),
        P("tp"),
        P("tp"),
        P(),
        P(("sp", "tp"), None),
        P(),
        P(("sp", "tp"), None),
        P(("sp", "tp"), None),
        P(("sp", "tp")),
        P(("sp", "tp"), None, None),
        P(("sp", "tp"), None, None),
        P(("sp", "tp"), None, None),
    )
    out_specs = P(("sp", "tp"), None)
    return jax.shard_map(local, mesh=mesh, in_specs=in_specs, out_specs=out_specs, check_vma=False)
```

```python
import functools

import jax
import jax.numpy as jnp
from jax import lax
from jax.experimental import pallas as pl
from jax.experimental.pallas import tpu as pltpu
from jax.sharding import PartitionSpec as P

CONV_GROUPS = 8


EPS = 1e-06


PLANES = 4
MESH = pl.DeviceIdType.MESH
ORDER = (1, 3, 2)
ROWS_MIN = 16
HALVES = 2


def layer_kernel(
    cap,
    slot,
    value_hbm,
    glu_gate_hbm,
    taps_hbm,
    bias_hbm,
    gain_hbm,
    shift_hbm,
    residual_hbm,
    ffn_hbm,
    pick_hbm,
    logit_hbm,
    prob_hbm,
    out_hbm,
    gate_hbm,
    up_hbm,
    down_hbm,
    out_ref,
    value_ref,
    gate_ref,
    taps_ref,
    bias_ref,
    gain_ref,
    shift_ref,
    residual_ref,
    ffn_ref,
    pick_ref,
    logit_ref,
    prob_ref,
    isem,
    glued,
    hsend,
    hrecv,
    mixed,
    mrest,
    place_ref,
    meta_ref,
    normed_ref,
    proj,
    out_v,
    zsend,
    zrecv,
    mrecv,
    xsend,
    xrecv,
    asend,
    arecv,
    csend,
    cret,
    gate_v,
    up_v,
    down_v,
    wsem,
    hss,
    hrs,
    tss,
    trs,
    zss,
    zrs,
    mss,
    mrs,
    xss,
    xrs,
    ass,
    ars,
    css,
    crs,
):
    n_tp = lax.axis_size("tp")
    chips = lax.axis_size("sp") // PLANES
    peers = chips * n_tp
    sp = lax.axis_index("sp")
    tp = lax.axis_index("tp")
    n_sp = lax.axis_size("sp")
    z = sp // chips
    here = sp % chips
    tokens = residual_ref.shape[0]
    length, channels = value_ref.shape
    reach = taps_ref.shape[0] - 1
    lead = hsend.shape[0]
    j = here * n_tp + tp
    slots = peers * slot
    group_rows = zsend.shape[2]
    half = zsend.shape[3]

    def span(h):
        return slice(h * half, (h + 1) * half)

    def plane(d):
        if d == 1:
            return z + 1 - 2 * (z % 2)
        if d == 2:
            return z + 2 - 4 * (z // 2)
        return PLANES - 1 - z

    def mate(d):
        return (plane(d) * chips + here, tp)

    def peer(k):
        return (z * chips + k // n_tp, k % n_tp)

    def zcopy(d, h):
        return pltpu.make_async_remote_copy(
            src_ref=zsend.at[d, h], dst_ref=zrecv.at[d, h],
            send_sem=zss.at[d, h], recv_sem=zrs.at[d, h],
            device_id=mate(d), device_id_type=MESH,
        )

    def mcopy(d):
        return pltpu.make_async_remote_copy(
            src_ref=meta_ref.at[d], dst_ref=mrecv.at[d], send_sem=mss.at[d], recv_sem=mrs.at[d],
            device_id=mate(d), device_id_type=MESH,
        )

    def ccopy(d, h):
        return pltpu.make_async_remote_copy(
            src_ref=csend.at[d, h], dst_ref=cret.at[d, h],
            send_sem=css.at[d, h], recv_sem=crs.at[d, h],
            device_id=mate(d), device_id_type=MESH,
        )

    def xcopy(d, h, o):
        rows = pl.ds(o * slot, slot)
        return pltpu.make_async_remote_copy(
            src_ref=xsend.at[d, h, rows], dst_ref=xrecv.at[d, h, rows],
            send_sem=xss.at[d, h, o], recv_sem=xrs.at[d, h, o],
            device_id=peer((j + o) % peers), device_id_type=MESH,
        )

    def acopy(d, h, o):
        rows = pl.ds(o * slot, slot)
        return pltpu.make_async_remote_copy(
            src_ref=asend.at[d, h, rows], dst_ref=arecv.at[d, h, rows],
            send_sem=ass.at[d, h, o], recv_sem=ars.at[d, h, o],
            device_id=peer((j + peers - o) % peers), device_id_type=MESH,
        )

    def halo():
        return pltpu.make_async_remote_copy(
            src_ref=hsend, dst_ref=hrecv, send_sem=hss.at[0], recv_sem=hrs.at[0],
            device_id=((sp + 1) % n_sp, tp), device_id_type=MESH,
        )

    wide_group = channels * n_tp // CONV_GROUPS
    block = 64

    def tcopy(o, begin, size):
        other = (tp + o) % n_tp
        rows = pl.ds(pl.multiple_of(other * tokens + begin, size), size)
        mark = begin // (block // 2)
        return pltpu.make_async_remote_copy(
            src_ref=mixed.at[rows], dst_ref=mrest.at[o, pl.ds(begin, size)],
            send_sem=tss.at[o, mark], recv_sem=trs.at[o, mark],
            device_id=(sp, other), device_id_type=MESH,
        )

    head_dev, tail_dev = sp == 0, sp == n_sp - 1
    barrier = pltpu.get_barrier_semaphore()
    inner = (z >= 1) & (z < PLANES - 1)
    outer = jnp.logical_not(inner)
    pl.semaphore_signal(barrier, inc=1, device_id=mate(1), device_id_type=MESH)

    @pl.when(inner)
    def _():
        pl.semaphore_signal(barrier, inc=1, device_id=mate(3), device_id_type=MESH)

    for o in range(1, peers):
        pl.semaphore_signal(
            barrier, inc=1, device_id=peer((j + o) % peers), device_id_type=MESH
        )

    @pl.when(jnp.logical_not(tail_dev))
    def _():
        pl.semaphore_signal(barrier, inc=1, device_id=(sp + 1, tp), device_id_type=MESH)

    @pl.when(jnp.logical_not(head_dev))
    def _():
        pl.semaphore_signal(barrier, inc=1, device_id=(sp - 1, tp), device_id_type=MESH)

    sources = (
        (value_hbm, value_ref), (glu_gate_hbm, gate_ref), (pick_hbm, pick_ref),
        (logit_hbm, logit_ref), (prob_hbm, prob_ref), (taps_hbm, taps_ref),
        (bias_hbm, bias_ref), (gain_hbm, gain_ref), (shift_hbm, shift_ref),
        (ffn_hbm, ffn_ref), (residual_hbm, residual_ref),
    )
    inputs = [pltpu.make_async_copy(a, b, isem.at[k]) for k, (a, b) in enumerate(sources)]
    for copy in inputs:
        copy.start()
    out_copy = pltpu.make_async_copy(out_hbm, out_v, wsem.at[3])
    weights = [
        pltpu.make_async_copy(gate_hbm.at[0], gate_v, wsem.at[0]),
        pltpu.make_async_copy(up_hbm.at[0], up_v, wsem.at[1]),
        pltpu.make_async_copy(down_hbm.at[0], down_v, wsem.at[2]),
    ]
    f32 = jnp.float32
    bf16 = jnp.bfloat16
    for copy in inputs[:2]:
        copy.wait()
    out_copy.start()
    for start in range(length - block, -1, -block):
        rows = slice(start, start + block)
        gated = value_ref[rows].astype(f32) / (1.0 + jnp.exp(-gate_ref[rows].astype(f32)))
        gated = gated.astype(bf16)
        for k in range(channels // wide_group):
            piece = gated[:, k * wide_group : (k + 1) * wide_group]
            glued[k, lead + start : lead + start + block] = piece.astype(f32)
        if start == length - block:
            hsend[...] = gated[block - lead :]
    for copy in inputs[2:5]:
        copy.wait()
    picks = pick_ref[...].astype(f32)
    logits = logit_ref[...]
    rows_of = [picks[0:1, :], picks[1:2, :], logits[0:1, :], logits[1:2, :]]
    sublane = lax.broadcasted_iota(jnp.int32, (128, tokens), 0)
    tall = jnp.zeros((128, tokens), f32)
    for k in range(2):
        tall = jnp.where(sublane == k, rows_of[k], tall)
    wide = tall.T
    cols = [wide[:, 0:1], wide[:, 1:2]]
    square = (tokens, tokens)
    earlier = lax.broadcasted_iota(jnp.int32, square, 0) < lax.broadcasted_iota(
        jnp.int32, square, 1
    )

    def group_of(pick):
        total = jnp.zeros(pick.shape, f32)
        for q in range(1, PLANES):
            total += jnp.where(pick >= (q * peers), 1.0, 0.0)
        return total

    def count(hit):
        return jnp.sum(jnp.where(hit & earlier, 1.0, 0.0), axis=0, keepdims=True)

    ranks = [count((cols[0] == r) | (cols[1] == r)) for r in rows_of[:2]]
    group_row = group_of(rows_of[0])
    spot = count(group_of(cols[0]) == group_row)
    away = group_row.astype(jnp.int32) ^ z
    at_row = away.astype(f32) * group_rows + spot
    row_id = lax.broadcasted_iota(jnp.int32, (PLANES * group_rows, tokens), 0).astype(f32)
    place_ref[...] = jnp.where(row_id == at_row, 1.0, 0.0).astype(bf16)
    gap = rows_of[2] - rows_of[3]
    shares = [prob_ref[...] / (1.0 + jnp.exp(-gap)), prob_ref[...] / (1.0 + jnp.exp(gap))]
    fields = [jnp.ones((1, tokens), f32)]
    for k in range(2):
        fields += [rows_of[k] - group_row * peers, ranks[k]]
    for share in shares:
        for _ in range(3):
            part = share.astype(bf16).astype(f32)
            fields.append(part)
            share = share - part
    field_id = lax.broadcasted_iota(jnp.int32, (16, tokens), 0)
    table = jnp.zeros((16, tokens), f32)
    for k, field in enumerate(fields):
        table = jnp.where(field_id == k, field, table)
    table = table.astype(bf16)
    meta_ref[...] = jnp.zeros(meta_ref.shape, f32)
    for d in range(PLANES):
        part = lax.dot_general(
            table,
            place_ref[d * group_rows : (d + 1) * group_rows, :],
            (((1,), (1,)), ((), ())),
            preferred_element_type=f32,
        )
        empty = (1.0 - part[0:1]) * 65536.0
        meta_ref[d, 0:1, :group_rows] = part[1:2] * slot + part[2:3] + empty
        meta_ref[d, 1:2, :group_rows] = part[3:4] * slot + part[4:5] + empty
        meta_ref[d, 2:3, :group_rows] = part[5:6] + part[6:7] + part[7:8]
        meta_ref[d, 3:4, :group_rows] = part[8:9] + part[9:10] + part[10:11]
    for copy in inputs[5:]:
        copy.wait()
    for copy in weights:
        copy.start()
    taps = taps_ref[...].astype(f32)
    def enter():
        pl.semaphore_wait(
            barrier,
            peers + jnp.where(inner, 1, 0)
            + jnp.where(head_dev, 0, 1) + jnp.where(tail_dev, 0, 1),
        )

        @pl.when(jnp.logical_not(tail_dev))
        def _():
            halo().start()

        mcopy(1).start()

        @pl.when(inner)
        def _():
            mcopy(3).start()

    spans = [(start, block) for start in range(length - block, 0, -block)]
    spans += [(block // 2, block // 2), (0, block // 2)]
    for start, size in spans:
        if start == length - block * 2:
            enter()

        if start == 0:

            @pl.when(head_dev)
            def _():
                glued[:, :lead] = jnp.zeros((channels // wide_group, lead, wide_group), f32)

            @pl.when(jnp.logical_not(head_dev))
            def _():
                halo().wait_recv()
                for k in range(channels // wide_group):
                    piece = hrecv[:, k * wide_group : (k + 1) * wide_group]
                    glued[k, :lead] = piece.astype(f32)

        for low_lane in range(0, channels, wide_group):
            part = slice(low_lane, low_lane + wide_group)
            total = jnp.zeros((size, wide_group), f32) + bias_ref[:, part]
            for offset in range(reach + 1):
                first = start + lead - reach + offset
                total += taps[offset : offset + 1, part] * glued[low_lane // wide_group, first : first + size]
            centre = jnp.mean(total, axis=-1, keepdims=True)
            total = total - centre
            variance = jnp.mean(total * total, axis=-1, keepdims=True)
            level = total * lax.rsqrt(variance + EPS)
            level = level * gain_ref[:, part] + shift_ref[:, part]
            mixed[start : start + size, part] = (level / (1.0 + jnp.exp(-level))).astype(bf16)
        if start + size == length:
            continue
        pieces = (start,) if start + size + block < length else (start, start + size)
        for piece in pieces:
            for o in range(1, n_tp):

                @pl.when((tp + o) % n_tp == piece // tokens)
                def _():
                    tcopy(o, piece % tokens, size).start()

    out_copy.wait()

    def weight_rows(which):
        return out_v[pl.ds(pl.multiple_of(which * channels, channels), channels), :]

    own = mixed[pl.ds(pl.multiple_of(tp * tokens, tokens), tokens), :]
    proj[...] = jnp.dot(own, weight_rows(tp), preferred_element_type=f32)

    def arrivals(act):
        for who in range(n_tp):
            for start, size in spans:
                if start // tokens == who:
                    for o in range(1, n_tp):
                        act(who, o, start % tokens, size)

    def landed(who, o, begin, size):
        @pl.when(tp == who)
        def _():
            tcopy(o, begin, size).wait_recv()

    def left(who, o, begin, size):
        @pl.when((tp + o) % n_tp == who)
        def _():
            tcopy(o, begin, size).wait_send()

    arrivals(landed)
    for o in range(1, n_tp):
        proj[...] += jnp.dot(
            mrest[o], weight_rows((tp + n_tp - o) % n_tp), preferred_element_type=f32
        )
    for start in range(0, tokens, 16):
        rows = slice(start, start + 16)
        hidden = (residual_ref[rows].astype(f32) + proj[rows]).astype(bf16)
        full = hidden.astype(f32)
        proj[rows] = full
        scale = lax.rsqrt(jnp.mean(full * full, axis=-1, keepdims=True) + EPS)
        normed_ref[rows] = (full * scale * ffn_ref[...]).astype(bf16)

    def places(d):
        meta = meta_ref[0] if d == 0 else mrecv[d]
        row = lax.broadcasted_iota(jnp.int32, (slots, group_rows), 0).astype(jnp.float32)
        shift = (j * slot).astype(jnp.float32)
        out = []
        for k in range(2):
            at = meta[k : k + 1, :group_rows] - shift
            at = jnp.where(at < 0, at + slots, at)
            out.append(row == at)
        shares = [meta[2 + k : 3 + k, :group_rows] for k in range(2)]
        return out, shares

    def chosen(d):
        at, _ = places(d)
        return jnp.where(at[0] | at[1], 1.0, 0.0).astype(jnp.bfloat16)

    def spread(d, h, pick):
        rows = zsend[0, h] if d == 0 else zrecv[d, h]
        wide = jnp.dot(pick, rows, preferred_element_type=jnp.float32)
        wide = wide.astype(jnp.bfloat16)
        xrecv[d, h, :slot] = wide[:slot]
        xsend[d, h, slot:] = wide[slot:]
        for o in range(1, peers):
            xcopy(d, h, o).start()

    def gather(d, h):
        picked = jnp.dot(
            place_ref[d * group_rows : (d + 1) * group_rows, :],
            normed_ref[:, span(h)],
            preferred_element_type=f32,
        )
        zsend[d, h] = picked.astype(bf16)

    def dispatch(d, h):
        gather(d, h)
        if d == 1:
            zcopy(d, h).start()
        elif d == 3:

            @pl.when(inner)
            def _():
                zcopy(d, h).start()

    own_pick = chosen(0)
    for h in range(HALVES):
        gather(0, h)
        spread(0, h, own_pick)
        dispatch(3, h)
        dispatch(1, h)
    for h in range(HALVES):
        dispatch(2, h)

    def entry(d, after=(), halves=tuple(range(HALVES))):
        if halves[0] == 0:
            mcopy(d).wait_recv()
        pick = chosen(d)
        for h in halves:
            zcopy(d, h).wait_recv()
            for who in range(n_tp if after else 0):
                if h == min(who, HALVES - 1):

                    @pl.when(tp == who)
                    def _():
                        for later in after:
                            mcopy(later).start()
                            for k in range(HALVES):
                                zcopy(later, k).start()

            spread(d, h, pick)

    def expert(d):
        gate_out = None
        for h in range(HALVES):
            for o in range(1, peers):
                xcopy(d, h, o).wait_recv()
            rows = xrecv[d, h]
            gate_part = jnp.dot(rows, gate_v[span(h), :], preferred_element_type=jnp.float32)
            up_part = jnp.dot(rows, up_v[span(h), :], preferred_element_type=jnp.float32)
            gate_out = gate_part if h == 0 else gate_out + gate_part
            up_out = up_part if h == 0 else up_out + up_part
        active = (gate_out / (1.0 + jnp.exp(-gate_out)) * up_out).astype(jnp.bfloat16)
        for h in range(HALVES):
            answer = jnp.dot(active, down_v[:, span(h)], preferred_element_type=jnp.float32)
            answer = answer.astype(jnp.bfloat16)
            arecv[d, h, :slot] = answer[:slot]
            asend[d, h, slot:] = answer[slot:]

    def reply(d, halves=tuple(range(HALVES))):
        for h in halves:
            for o in range(1, peers):
                acopy(d, h, o).start()

    def settle(d, h, last=False):
        if d:
            ccopy(d, h).wait_recv()
        total = lax.dot_general(
            place_ref[d * group_rows : (d + 1) * group_rows, :],
            cret[d, h],
            (((0,), (0,)), ((), ())),
            preferred_element_type=f32,
        )
        total += proj[:, span(h)]
        if last:
            out_ref[:, span(h)] = total.astype(bf16)
        else:
            proj[:, span(h)] = total

    def combine(d, halves=tuple(range(HALVES))):
        at, shares = places(d)
        mix = jnp.where(at[0], shares[0], 0.0) + jnp.where(at[1], shares[1], 0.0)
        high = mix.astype(jnp.bfloat16)
        low = (mix - high.astype(jnp.float32)).astype(jnp.bfloat16)
        dims = (((0,), (0,)), ((), ()))
        for h in halves:
            for o in range(1, peers):
                acopy(d, h, o).wait_recv()
            answers = arecv[d, h]
            total = lax.dot_general(high, answers, dims, preferred_element_type=jnp.float32)
            total += lax.dot_general(low, answers, dims, preferred_element_type=jnp.float32)
            if d == 0:
                cret[0, h] = total.astype(jnp.bfloat16)
            else:
                csend[d, h] = total.astype(jnp.bfloat16)
                ccopy(d, h).start()

    def drain():
        @pl.when(jnp.logical_not(tail_dev))
        def _():
            halo().wait_send()

        arrivals(left)
        for d in ORDER:
            mcopy(d).wait_send()
            for h in range(HALVES):
                zcopy(d, h).wait_send()
        for d in range(PLANES):
            for h in range(HALVES):
                for o in range(1, peers):
                    xcopy(d, h, o).wait_send()
                    acopy(d, h, o).wait_send()

    head, rest = (0,), tuple(range(1, HALVES))

    @pl.when(inner)
    def _():
        entry(3, after=(2,))
        entry(1)
        for copy in weights:
            copy.wait()
        expert(0)
        expert(3)
        reply(3)
        expert(1)
        reply(1, head)
        combine(3)
        entry(2)
        reply(1, rest)
        combine(1, head)
        expert(2)
        reply(2)
        combine(1, rest)
        combine(2, head)
        reply(0)
        combine(2, rest)
        for h in range(HALVES):
            settle(3, h)
        for h in range(HALVES):
            combine(0, (h,))
            settle(0, h)
        drain()
        for h in range(HALVES):
            settle(1, h)
        for h in range(HALVES):
            settle(2, h, last=True)

    @pl.when(outer)
    def _():
        entry(1)
        for copy in weights:
            copy.wait()
        expert(0)
        entry(2, after=(3, 2))
        expert(1)
        entry(3)
        reply(1, head)
        expert(2)
        reply(2, head)
        expert(3)
        reply(3)
        combine(1, head)
        combine(2, head)
        reply(1, rest)
        reply(0, head)
        combine(3)
        reply(2, rest)
        combine(1, rest)
        reply(0, rest)
        combine(0, head)
        combine(2, rest)
        settle(0, 0)
        combine(0, rest)
        for h in rest:
            settle(0, h)
        drain()
        for h in range(HALVES):
            settle(3, h)
            settle(1, h)
        for h in range(HALVES):
            settle(2, h, last=True)

    for d in ORDER:
        for h in range(HALVES):
            ccopy(d, h).wait_send()


def local(
    glu_value,
    glu_gate,
    conv_kernel,
    conv_bias,
    group_gain,
    group_shift,
    out_weight,
    residual,
    ffn_gain,
    expert_pick,
    pair_logits,
    group_prob,
    gate_weight,
    up_weight,
    down_weight,
):
    rows, width = residual.shape
    length, channels = glu_value.shape
    n_tp = lax.axis_size("tp")
    experts_all = lax.axis_size("sp") * n_tp
    cap = 4 * rows // experts_all
    peers = experts_all // PLANES
    group_rows = peers * cap // 2
    slot = max(cap, ROWS_MIN)
    slots = peers * slot
    wide_group = channels * n_tp // CONV_GROUPS
    lead = -(-(conv_kernel.shape[0] - 1) // 16) * 16
    bf16 = jnp.bfloat16
    f32 = jnp.float32
    vmem = pl.BlockSpec(memory_space=pltpu.VMEM)
    hbm = pl.BlockSpec(memory_space=pl.ANY)
    dma = pltpu.SemaphoreType.DMA
    return pl.pallas_call(
        functools.partial(layer_kernel, cap, slot),
        out_shape=pltpu.VMEM((rows, width), bf16),
        in_specs=[hbm] * 15,
        out_specs=vmem,
        scratch_shapes=[
            pltpu.VMEM(glu_value.shape, bf16),
            pltpu.VMEM(glu_gate.shape, bf16),
            pltpu.VMEM(conv_kernel.shape, bf16),
            pltpu.VMEM((1, channels), f32),
            pltpu.VMEM((1, channels), f32),
            pltpu.VMEM((1, channels), f32),
            pltpu.VMEM((rows, width), bf16),
            pltpu.VMEM((1, width), f32),
            pltpu.VMEM((2, rows), jnp.int32),
            pltpu.VMEM((2, rows), f32),
            pltpu.VMEM((1, rows), f32),
            dma((11,)),
            pltpu.VMEM((channels // wide_group, lead + length, wide_group), f32),
            pltpu.VMEM((lead, channels), bf16),
            pltpu.VMEM((lead, channels), bf16),
            pltpu.VMEM((length, channels), bf16),
            pltpu.VMEM((n_tp, rows, channels), bf16),
            pltpu.VMEM((PLANES * group_rows, rows), bf16),
            pltpu.VMEM((PLANES, 8, 128), f32),
            pltpu.VMEM((rows, width), bf16),
            pltpu.VMEM((rows, width), f32),
            pltpu.VMEM(out_weight.shape, bf16),
            pltpu.VMEM((PLANES, HALVES, group_rows, width // HALVES), bf16),
            pltpu.VMEM((PLANES, HALVES, group_rows, width // HALVES), bf16),
            pltpu.VMEM((PLANES, 8, 128), f32),
            pltpu.VMEM((PLANES, HALVES, slots, width // HALVES), bf16),
            pltpu.VMEM((PLANES, HALVES, slots, width // HALVES), bf16),
            pltpu.VMEM((PLANES, HALVES, slots, width // HALVES), bf16),
            pltpu.VMEM((PLANES, HALVES, slots, width // HALVES), bf16),
            pltpu.VMEM((PLANES, HALVES, group_rows, width // HALVES), bf16),
            pltpu.VMEM((PLANES, HALVES, group_rows, width // HALVES), bf16),
            pltpu.VMEM(gate_weight.shape[1:], bf16),
            pltpu.VMEM(up_weight.shape[1:], bf16),
            pltpu.VMEM(down_weight.shape[1:], bf16),
            dma((4,)),
            dma((1,)),
            dma((1,)),
            dma((n_tp, rows // 32)),
            dma((n_tp, rows // 32)),
            dma((PLANES, HALVES)),
            dma((PLANES, HALVES)),
            dma((PLANES,)),
            dma((PLANES,)),
            dma((PLANES, HALVES, peers)),
            dma((PLANES, HALVES, peers)),
            dma((PLANES, HALVES, peers)),
            dma((PLANES, HALVES, peers)),
            dma((PLANES, HALVES)),
            dma((PLANES, HALVES)),
        ],
        compiler_params=pltpu.CompilerParams(
            collective_id=0, has_side_effects=True, vmem_limit_bytes=62 * 1024 * 1024
        ),
    )(
        glu_value,
        glu_gate,
        conv_kernel,
        conv_bias[None, :],
        group_gain[None, :],
        group_shift[None, :],
        residual,
        ffn_gain[None, :],
        expert_pick.T,
        pair_logits.T,
        group_prob[None, :],
        out_weight,
        gate_weight,
        up_weight,
        down_weight,
    )


def solution(mesh):
    in_specs = (
        P("sp", "tp"),
        P("sp", "tp"),
        P(None, "tp"),
        P("tp"),
        P("tp"),
        P("tp"),
        P(),
        P(("sp", "tp"), None),
        P(),
        P(("sp", "tp"), None),
        P(("sp", "tp"), None),
        P(("sp", "tp")),
        P(("sp", "tp"), None, None),
        P(("sp", "tp"), None, None),
        P(("sp", "tp"), None, None),
    )
    out_specs = P(("sp", "tp"), None)
    return jax.shard_map(local, mesh=mesh, in_specs=in_specs, out_specs=out_specs, check_vma=False)
```

```python
import functools

import jax
import jax.numpy as jnp
from jax import lax
from jax.experimental import pallas as pl
from jax.experimental.pallas import tpu as pltpu
from jax.sharding import PartitionSpec as P

CONV_GROUPS = 8


EPS = 1e-06


PLANES = 4
MESH = pl.DeviceIdType.MESH
ORDER = (1, 3, 2)
ROWS_MIN = 16
HALVES = 2


def layer_kernel(
    cap,
    slot,
    value_hbm,
    glu_gate_hbm,
    taps_hbm,
    bias_hbm,
    gain_hbm,
    shift_hbm,
    residual_hbm,
    ffn_hbm,
    pick_hbm,
    logit_hbm,
    prob_hbm,
    out_hbm,
    gate_hbm,
    up_hbm,
    down_hbm,
    out_ref,
    value_ref,
    gate_ref,
    taps_ref,
    bias_ref,
    gain_ref,
    shift_ref,
    residual_ref,
    ffn_ref,
    pick_ref,
    logit_ref,
    prob_ref,
    isem,
    glued,
    hsend,
    hrecv,
    mixed,
    mrest,
    place_ref,
    meta_ref,
    normed_ref,
    proj,
    out_v,
    zsend,
    zrecv,
    mrecv,
    xsend,
    xrecv,
    asend,
    arecv,
    csend,
    cret,
    gate_v,
    up_v,
    down_v,
    hss,
    hrs,
    tss,
    trs,
    zss,
    zrs,
    mss,
    mrs,
    xss,
    xrs,
    ass,
    ars,
    css,
    crs,
):
    n_tp = lax.axis_size("tp")
    chips = lax.axis_size("sp") // PLANES
    peers = chips * n_tp
    sp = lax.axis_index("sp")
    tp = lax.axis_index("tp")
    n_sp = lax.axis_size("sp")
    z = sp // chips
    here = sp % chips
    tokens = residual_ref.shape[0]
    length, channels = value_ref.shape
    reach = taps_ref.shape[0] - 1
    lead = hsend.shape[0]
    j = here * n_tp + tp
    slots = peers * slot
    group_rows = zsend.shape[2]
    half = zsend.shape[3]

    def span(h):
        return slice(h * half, (h + 1) * half)

    def plane(d):
        if d == 1:
            return z + 1 - 2 * (z % 2)
        if d == 2:
            return z + 2 - 4 * (z // 2)
        return PLANES - 1 - z

    def mate(d):
        return (plane(d) * chips + here, tp)

    def peer(k):
        return (z * chips + k // n_tp, k % n_tp)

    def zcopy(d, h):
        return pltpu.make_async_remote_copy(
            src_ref=zsend.at[d, h], dst_ref=zrecv.at[d, h],
            send_sem=zss.at[0], recv_sem=zrs.at[d - 1, h],
            device_id=mate(d), device_id_type=MESH,
        )

    def mcopy(d):
        return pltpu.make_async_remote_copy(
            src_ref=meta_ref.at[d], dst_ref=mrecv.at[d], send_sem=mss.at[0], recv_sem=mrs.at[d - 1],
            device_id=mate(d), device_id_type=MESH,
        )

    def ccopy(d, h):
        return pltpu.make_async_remote_copy(
            src_ref=csend.at[d, h], dst_ref=cret.at[d, h],
            send_sem=css.at[0], recv_sem=crs.at[d - 1, h],
            device_id=mate(d), device_id_type=MESH,
        )

    def xcopy(d, h, o):
        rows = pl.ds(o * slot, slot)
        return pltpu.make_async_remote_copy(
            src_ref=xsend.at[d, h, rows], dst_ref=xrecv.at[d, h, rows],
            send_sem=xss.at[0], recv_sem=xrs.at[d, h],
            device_id=peer((j + o) % peers), device_id_type=MESH,
        )

    def xall(d, h):
        rows = pl.ds(slot, slots - slot)
        return pltpu.make_async_remote_copy(
            src_ref=xsend.at[d, h, rows], dst_ref=xrecv.at[d, h, rows],
            send_sem=xss.at[0], recv_sem=xrs.at[d, h],
            device_id=peer((j + 1) % peers), device_id_type=MESH,
        )

    def acopy(d, h, o):
        rows = pl.ds(o * slot, slot)
        return pltpu.make_async_remote_copy(
            src_ref=asend.at[d, h, rows], dst_ref=arecv.at[d, h, rows],
            send_sem=ass.at[0], recv_sem=ars.at[d, h],
            device_id=peer((j + peers - o) % peers), device_id_type=MESH,
        )

    def aall(d, h):
        rows = pl.ds(slot, slots - slot)
        return pltpu.make_async_remote_copy(
            src_ref=asend.at[d, h, rows], dst_ref=arecv.at[d, h, rows],
            send_sem=ass.at[0], recv_sem=ars.at[d, h],
            device_id=peer((j + peers - 1) % peers), device_id_type=MESH,
        )

    def sent(src, sem, recv_sem):
        return pltpu.make_async_remote_copy(
            src_ref=src, dst_ref=src, send_sem=sem.at[0], recv_sem=recv_sem,
            device_id=mate(1), device_id_type=MESH,
        )

    def halo():
        return pltpu.make_async_remote_copy(
            src_ref=hsend, dst_ref=hrecv, send_sem=hss.at[0], recv_sem=hrs.at[0],
            device_id=((sp + 1) % n_sp, tp), device_id_type=MESH,
        )

    wide_group = channels * n_tp // CONV_GROUPS
    block = 64

    def tcopy(o, begin, size):
        other = (tp + o) % n_tp
        rows = pl.ds(pl.multiple_of(other * tokens + begin, size), size)
        return pltpu.make_async_remote_copy(
            src_ref=mixed.at[rows], dst_ref=mrest.at[o, pl.ds(begin, size)],
            send_sem=tss.at[o - 1], recv_sem=trs.at[o - 1],
            device_id=(sp, other), device_id_type=MESH,
        )

    head_dev, tail_dev = sp == 0, sp == n_sp - 1
    barrier = pltpu.get_barrier_semaphore()
    inner = (z >= 1) & (z < PLANES - 1)
    outer = jnp.logical_not(inner)
    pl.semaphore_signal(barrier, inc=1, device_id=mate(1), device_id_type=MESH)

    @pl.when(inner)
    def _():
        pl.semaphore_signal(barrier, inc=1, device_id=mate(3), device_id_type=MESH)

    for o in range(1, peers):
        pl.semaphore_signal(
            barrier, inc=1, device_id=peer((j + o) % peers), device_id_type=MESH
        )

    @pl.when(jnp.logical_not(tail_dev))
    def _():
        pl.semaphore_signal(barrier, inc=1, device_id=(sp + 1, tp), device_id_type=MESH)

    @pl.when(jnp.logical_not(head_dev))
    def _():
        pl.semaphore_signal(barrier, inc=1, device_id=(sp - 1, tp), device_id_type=MESH)

    sources = (
        (value_hbm, value_ref), (glu_gate_hbm, gate_ref), (pick_hbm, pick_ref),
        (logit_hbm, logit_ref), (prob_hbm, prob_ref), (taps_hbm, taps_ref),
        (bias_hbm, bias_ref), (gain_hbm, gain_ref), (shift_hbm, shift_ref),
        (ffn_hbm, ffn_ref), (residual_hbm, residual_ref),
    )
    inputs = [pltpu.make_async_copy(a, b, isem.at[k]) for k, (a, b) in enumerate(sources)]
    for copy in inputs:
        copy.start()
    out_copy = pltpu.make_async_copy(out_hbm, out_v, isem.at[0])
    weights = [
        pltpu.make_async_copy(gate_hbm.at[0], gate_v, isem.at[5]),
        pltpu.make_async_copy(up_hbm.at[0], up_v, isem.at[6]),
        pltpu.make_async_copy(down_hbm.at[0], down_v, isem.at[7]),
    ]
    f32 = jnp.float32
    bf16 = jnp.bfloat16
    for copy in inputs[:2]:
        copy.wait()
    out_copy.start()
    for start in range(length - block, -1, -block):
        rows = slice(start, start + block)
        gated = value_ref[rows].astype(f32) / (1.0 + jnp.exp(-gate_ref[rows].astype(f32)))
        gated = gated.astype(bf16)
        for k in range(channels // wide_group):
            piece = gated[:, k * wide_group : (k + 1) * wide_group]
            glued[k, lead + start : lead + start + block] = piece.astype(f32)
        if start == length - block:
            hsend[...] = gated[block - lead :]
    for copy in inputs[2:5]:
        copy.wait()
    picks = pick_ref[...].astype(f32)
    logits = logit_ref[...]
    rows_of = [picks[0:1, :], picks[1:2, :], logits[0:1, :], logits[1:2, :]]
    sublane = lax.broadcasted_iota(jnp.int32, (128, tokens), 0)
    tall = jnp.zeros((128, tokens), f32)
    for k in range(2):
        tall = jnp.where(sublane == k, rows_of[k], tall)
    wide = tall.T
    cols = [wide[:, 0:1], wide[:, 1:2]]
    square = (tokens, tokens)
    earlier = lax.broadcasted_iota(jnp.int32, square, 0) < lax.broadcasted_iota(
        jnp.int32, square, 1
    )

    def group_of(pick):
        total = jnp.zeros(pick.shape, f32)
        for q in range(1, PLANES):
            total += jnp.where(pick >= (q * peers), 1.0, 0.0)
        return total

    def count(hit):
        return jnp.sum(jnp.where(hit & earlier, 1.0, 0.0), axis=0, keepdims=True)

    ranks = [count((cols[0] == r) | (cols[1] == r)) for r in rows_of[:2]]
    group_row = group_of(rows_of[0])
    spot = count(group_of(cols[0]) == group_row)
    away = group_row.astype(jnp.int32) ^ z
    at_row = away.astype(f32) * group_rows + spot
    row_id = lax.broadcasted_iota(jnp.int32, (PLANES * group_rows, tokens), 0).astype(f32)
    place_ref[...] = jnp.where(row_id == at_row, 1.0, 0.0).astype(bf16)
    gap = rows_of[2] - rows_of[3]
    shares = [prob_ref[...] / (1.0 + jnp.exp(-gap)), prob_ref[...] / (1.0 + jnp.exp(gap))]
    fields = [jnp.ones((1, tokens), f32)]
    for k in range(2):
        fields += [rows_of[k] - group_row * peers, ranks[k]]
    for share in shares:
        for _ in range(3):
            part = share.astype(bf16).astype(f32)
            fields.append(part)
            share = share - part
    field_id = lax.broadcasted_iota(jnp.int32, (16, tokens), 0)
    table = jnp.zeros((16, tokens), f32)
    for k, field in enumerate(fields):
        table = jnp.where(field_id == k, field, table)
    table = table.astype(bf16)
    meta_ref[...] = jnp.zeros(meta_ref.shape, f32)
    for d in range(PLANES):
        part = lax.dot_general(
            table,
            place_ref[d * group_rows : (d + 1) * group_rows, :],
            (((1,), (1,)), ((), ())),
            preferred_element_type=f32,
        )
        empty = (1.0 - part[0:1]) * 65536.0
        meta_ref[d, 0:1, :group_rows] = part[1:2] * slot + part[2:3] + empty
        meta_ref[d, 1:2, :group_rows] = part[3:4] * slot + part[4:5] + empty
        meta_ref[d, 2:3, :group_rows] = part[5:6] + part[6:7] + part[7:8]
        meta_ref[d, 3:4, :group_rows] = part[8:9] + part[9:10] + part[10:11]
    for copy in inputs[5:]:
        copy.wait()
    for copy in weights:
        copy.start()
    taps = taps_ref[...].astype(f32)
    def enter():
        pl.semaphore_wait(
            barrier,
            peers + jnp.where(inner, 1, 0)
            + jnp.where(head_dev, 0, 1) + jnp.where(tail_dev, 0, 1),
        )

        @pl.when(jnp.logical_not(tail_dev))
        def _():
            halo().start()

        mcopy(1).start()

        @pl.when(inner)
        def _():
            mcopy(3).start()

    spans = [(start, block) for start in range(length - block, 0, -block)]
    spans += [(block // 2, block // 2), (0, block // 2)]
    for start, size in spans:
        if start == length - block * 2:
            enter()

        if start == 0:

            @pl.when(head_dev)
            def _():
                glued[:, :lead] = jnp.zeros((channels // wide_group, lead, wide_group), f32)

            @pl.when(jnp.logical_not(head_dev))
            def _():
                halo().wait_recv()
                for k in range(channels // wide_group):
                    piece = hrecv[:, k * wide_group : (k + 1) * wide_group]
                    glued[k, :lead] = piece.astype(f32)

        for low_lane in range(0, channels, wide_group):
            part = slice(low_lane, low_lane + wide_group)
            total = jnp.zeros((size, wide_group), f32) + bias_ref[:, part]
            for offset in range(reach + 1):
                first = start + lead - reach + offset
                total += taps[offset : offset + 1, part] * glued[low_lane // wide_group, first : first + size]
            centre = jnp.mean(total, axis=-1, keepdims=True)
            total = total - centre
            variance = jnp.mean(total * total, axis=-1, keepdims=True)
            level = total * lax.rsqrt(variance + EPS)
            level = level * gain_ref[:, part] + shift_ref[:, part]
            mixed[start : start + size, part] = (level / (1.0 + jnp.exp(-level))).astype(bf16)
        if start + size == length:
            continue
        pieces = (start,) if start + size + block < length else (start, start + size)
        for piece in pieces:
            for o in range(1, n_tp):

                @pl.when((tp + o) % n_tp == piece // tokens)
                def _():
                    tcopy(o, piece % tokens, size).start()

    out_copy.wait()

    def weight_rows(which):
        return out_v[pl.ds(pl.multiple_of(which * channels, channels), channels), :]

    own = mixed[pl.ds(pl.multiple_of(tp * tokens, tokens), tokens), :]
    proj[...] = jnp.dot(own, weight_rows(tp), preferred_element_type=f32)

    for o in range(1, n_tp):
        tcopy(o, 0, tokens).wait_recv()
    for o in range(1, n_tp):
        proj[...] += jnp.dot(
            mrest[o], weight_rows((tp + n_tp - o) % n_tp), preferred_element_type=f32
        )
    for start in range(0, tokens, 16):
        rows = slice(start, start + 16)
        hidden = (residual_ref[rows].astype(f32) + proj[rows]).astype(bf16)
        full = hidden.astype(f32)
        proj[rows] = full
        scale = lax.rsqrt(jnp.mean(full * full, axis=-1, keepdims=True) + EPS)
        normed_ref[rows] = (full * scale * ffn_ref[...]).astype(bf16)

    def places(d):
        meta = meta_ref[0] if d == 0 else mrecv[d]
        row = lax.broadcasted_iota(jnp.int32, (slots, group_rows), 0).astype(jnp.float32)
        shift = (j * slot).astype(jnp.float32)
        out = []
        for k in range(2):
            at = meta[k : k + 1, :group_rows] - shift
            at = jnp.where(at < 0, at + slots, at)
            out.append(row == at)
        shares = [meta[2 + k : 3 + k, :group_rows] for k in range(2)]
        return out, shares

    def chosen(d):
        at, _ = places(d)
        return jnp.where(at[0] | at[1], 1.0, 0.0).astype(jnp.bfloat16)

    def spread(d, h, pick):
        rows = zsend[0, h] if d == 0 else zrecv[d, h]
        wide = jnp.dot(pick, rows, preferred_element_type=jnp.float32)
        wide = wide.astype(jnp.bfloat16)
        xrecv[d, h, :slot] = wide[:slot]
        xsend[d, h, slot:] = wide[slot:]
        for o in range(1, peers):
            xcopy(d, h, o).start()

    def gather(d, h):
        picked = jnp.dot(
            place_ref[d * group_rows : (d + 1) * group_rows, :],
            normed_ref[:, span(h)],
            preferred_element_type=f32,
        )
        zsend[d, h] = picked.astype(bf16)

    def dispatch(d, h):
        gather(d, h)
        if d == 1:
            zcopy(d, h).start()
        elif d == 3:

            @pl.when(inner)
            def _():
                zcopy(d, h).start()

    own_pick = chosen(0)
    for h in range(HALVES):
        gather(0, h)
        spread(0, h, own_pick)
        dispatch(3, h)
        dispatch(1, h)
    for h in range(HALVES):
        dispatch(2, h)

    def entry(d, after=(), halves=tuple(range(HALVES))):
        if halves[0] == 0:
            mcopy(d).wait_recv()
        pick = chosen(d)
        for h in halves:
            zcopy(d, h).wait_recv()
            for who in range(n_tp if after else 0):
                if h == min(who, HALVES - 1):

                    @pl.when(tp == who)
                    def _():
                        for later in after:
                            mcopy(later).start()
                            for k in range(HALVES):
                                zcopy(later, k).start()

            spread(d, h, pick)

    def expert(d):
        gate_out = None
        for h in range(HALVES):
            xall(d, h).wait_recv()
            rows = xrecv[d, h]
            gate_part = jnp.dot(rows, gate_v[span(h), :], preferred_element_type=jnp.float32)
            up_part = jnp.dot(rows, up_v[span(h), :], preferred_element_type=jnp.float32)
            gate_out = gate_part if h == 0 else gate_out + gate_part
            up_out = up_part if h == 0 else up_out + up_part
        active = (gate_out / (1.0 + jnp.exp(-gate_out)) * up_out).astype(jnp.bfloat16)
        for h in range(HALVES):
            answer = jnp.dot(active, down_v[:, span(h)], preferred_element_type=jnp.float32)
            answer = answer.astype(jnp.bfloat16)
            arecv[d, h, :slot] = answer[:slot]
            asend[d, h, slot:] = answer[slot:]

    def reply(d, halves=tuple(range(HALVES))):
        for h in halves:
            for o in range(1, peers):
                acopy(d, h, o).start()

    def settle(d, h, last=False):
        if d:
            ccopy(d, h).wait_recv()
        total = lax.dot_general(
            place_ref[d * group_rows : (d + 1) * group_rows, :],
            cret[d, h],
            (((0,), (0,)), ((), ())),
            preferred_element_type=f32,
        )
        total += proj[:, span(h)]
        if last:
            out_ref[:, span(h)] = total.astype(bf16)
        else:
            proj[:, span(h)] = total

    def combine(d, halves=tuple(range(HALVES))):
        at, shares = places(d)
        mix = jnp.where(at[0], shares[0], 0.0) + jnp.where(at[1], shares[1], 0.0)
        high = mix.astype(jnp.bfloat16)
        low = (mix - high.astype(jnp.float32)).astype(jnp.bfloat16)
        dims = (((0,), (0,)), ((), ()))
        for h in halves:
            aall(d, h).wait_recv()
            answers = arecv[d, h]
            total = lax.dot_general(high, answers, dims, preferred_element_type=jnp.float32)
            total += lax.dot_general(low, answers, dims, preferred_element_type=jnp.float32)
            if d == 0:
                cret[0, h] = total.astype(jnp.bfloat16)
            else:
                csend[d, h] = total.astype(jnp.bfloat16)
                ccopy(d, h).start()

    def drain():
        @pl.when(jnp.logical_not(tail_dev))
        def _():
            halo().wait_send()

        for o in range(1, n_tp):
            tcopy(o, 0, tokens).wait_send()
        away = pl.ds(1, PLANES - 1)
        rows = pl.ds(slot, slots - slot)
        every = pl.ds(0, HALVES)
        sent(meta_ref.at[away], mss, mrs.at[0]).wait_send()
        sent(zsend.at[away], zss, zrs.at[0, 0]).wait_send()
        sent(xsend.at[pl.ds(0, PLANES), every, rows], xss, xrs.at[0, 0]).wait_send()
        sent(asend.at[pl.ds(0, PLANES), every, rows], ass, ars.at[0, 0]).wait_send()

    head, rest = (0,), tuple(range(1, HALVES))

    @pl.when(inner)
    def _():
        entry(3, after=(2,))
        entry(1)
        for copy in weights:
            copy.wait()
        expert(0)
        expert(3)
        reply(3)
        expert(1)
        reply(1, head)
        combine(3)
        entry(2)
        reply(1, rest)
        combine(1, head)
        expert(2)
        reply(2)
        combine(1, rest)
        combine(2, head)
        reply(0)
        combine(2, rest)
        for h in range(HALVES):
            settle(3, h)
        for h in range(HALVES):
            combine(0, (h,))
            settle(0, h)
        drain()
        for h in range(HALVES):
            settle(1, h)
        for h in range(HALVES):
            settle(2, h, last=True)

    @pl.when(outer)
    def _():
        entry(1)
        for copy in weights:
            copy.wait()
        expert(0)
        entry(2, after=(3, 2))
        expert(1)
        entry(3)
        reply(1, head)
        expert(2)
        reply(2, head)
        expert(3)
        reply(3)
        combine(1, head)
        combine(2, head)
        reply(1, rest)
        reply(0, head)
        combine(3)
        reply(2, rest)
        combine(1, rest)
        reply(0, rest)
        combine(0, head)
        combine(2, rest)
        settle(0, 0)
        combine(0, rest)
        for h in rest:
            settle(0, h)
        drain()
        for h in range(HALVES):
            settle(3, h)
            settle(1, h)
        for h in range(HALVES):
            settle(2, h, last=True)

    sent(csend.at[pl.ds(1, PLANES - 1)], css, crs.at[0, 0]).wait_send()


def local(
    glu_value,
    glu_gate,
    conv_kernel,
    conv_bias,
    group_gain,
    group_shift,
    out_weight,
    residual,
    ffn_gain,
    expert_pick,
    pair_logits,
    group_prob,
    gate_weight,
    up_weight,
    down_weight,
):
    rows, width = residual.shape
    length, channels = glu_value.shape
    n_tp = lax.axis_size("tp")
    experts_all = lax.axis_size("sp") * n_tp
    cap = 4 * rows // experts_all
    peers = experts_all // PLANES
    group_rows = peers * cap // 2
    slot = max(cap, ROWS_MIN)
    slots = peers * slot
    wide_group = channels * n_tp // CONV_GROUPS
    lead = -(-(conv_kernel.shape[0] - 1) // 16) * 16
    bf16 = jnp.bfloat16
    f32 = jnp.float32
    vmem = pl.BlockSpec(memory_space=pltpu.VMEM)
    hbm = pl.BlockSpec(memory_space=pl.ANY)
    dma = pltpu.SemaphoreType.DMA
    return pl.pallas_call(
        functools.partial(layer_kernel, cap, slot),
        out_shape=pltpu.VMEM((rows, width), bf16),
        in_specs=[hbm] * 15,
        out_specs=vmem,
        scratch_shapes=[
            pltpu.VMEM(glu_value.shape, bf16),
            pltpu.VMEM(glu_gate.shape, bf16),
            pltpu.VMEM(conv_kernel.shape, bf16),
            pltpu.VMEM((1, channels), f32),
            pltpu.VMEM((1, channels), f32),
            pltpu.VMEM((1, channels), f32),
            pltpu.VMEM((rows, width), bf16),
            pltpu.VMEM((1, width), f32),
            pltpu.VMEM((2, rows), jnp.int32),
            pltpu.VMEM((2, rows), f32),
            pltpu.VMEM((1, rows), f32),
            dma((11,)),
            pltpu.VMEM((channels // wide_group, lead + length, wide_group), f32),
            pltpu.VMEM((lead, channels), bf16),
            pltpu.VMEM((lead, channels), bf16),
            pltpu.VMEM((length, channels), bf16),
            pltpu.VMEM((n_tp, rows, channels), bf16),
            pltpu.VMEM((PLANES * group_rows, rows), bf16),
            pltpu.VMEM((PLANES, 8, 128), f32),
            pltpu.VMEM((rows, width), bf16),
            pltpu.VMEM((rows, width), f32),
            pltpu.VMEM(out_weight.shape, bf16),
            pltpu.VMEM((PLANES, HALVES, group_rows, width // HALVES), bf16),
            pltpu.VMEM((PLANES, HALVES, group_rows, width // HALVES), bf16),
            pltpu.VMEM((PLANES, 8, 128), f32),
            pltpu.VMEM((PLANES, HALVES, slots, width // HALVES), bf16),
            pltpu.VMEM((PLANES, HALVES, slots, width // HALVES), bf16),
            pltpu.VMEM((PLANES, HALVES, slots, width // HALVES), bf16),
            pltpu.VMEM((PLANES, HALVES, slots, width // HALVES), bf16),
            pltpu.VMEM((PLANES, HALVES, group_rows, width // HALVES), bf16),
            pltpu.VMEM((PLANES, HALVES, group_rows, width // HALVES), bf16),
            pltpu.VMEM(gate_weight.shape[1:], bf16),
            pltpu.VMEM(up_weight.shape[1:], bf16),
            pltpu.VMEM(down_weight.shape[1:], bf16),
            dma((1,)),
            dma((1,)),
            dma((n_tp - 1,)),
            dma((n_tp - 1,)),
            dma((1,)),
            dma((PLANES - 1, HALVES)),
            dma((1,)),
            dma((PLANES - 1,)),
            dma((1,)),
            dma((PLANES, HALVES)),
            dma((1,)),
            dma((PLANES, HALVES)),
            dma((1,)),
            dma((PLANES - 1, HALVES)),
        ],
        compiler_params=pltpu.CompilerParams(
            collective_id=0, has_side_effects=True, vmem_limit_bytes=62 * 1024 * 1024
        ),
    )(
        glu_value,
        glu_gate,
        conv_kernel,
        conv_bias[None, :],
        group_gain[None, :],
        group_shift[None, :],
        residual,
        ffn_gain[None, :],
        expert_pick.T,
        pair_logits.T,
        group_prob[None, :],
        out_weight,
        gate_weight,
        up_weight,
        down_weight,
    )


def solution(mesh):
    in_specs = (
        P("sp", "tp"),
        P("sp", "tp"),
        P(None, "tp"),
        P("tp"),
        P("tp"),
        P("tp"),
        P(),
        P(("sp", "tp"), None),
        P(),
        P(("sp", "tp"), None),
        P(("sp", "tp"), None),
        P(("sp", "tp")),
        P(("sp", "tp"), None, None),
        P(("sp", "tp"), None, None),
        P(("sp", "tp"), None, None),
    )
    out_specs = P(("sp", "tp"), None)
    return jax.shard_map(local, mesh=mesh, in_specs=in_specs, out_specs=out_specs, check_vma=False)
```

```python
import functools

import jax
import jax.numpy as jnp
from jax import lax
from jax.experimental import pallas as pl
from jax.experimental.pallas import tpu as pltpu
from jax.sharding import PartitionSpec as P

CONV_GROUPS = 8


EPS = 1e-06


PLANES = 4
MESH = pl.DeviceIdType.MESH
ORDER = (1, 3, 2)
ROWS_MIN = 16
HALVES = 2


def layer_kernel(
    cap,
    slot,
    value_hbm,
    glu_gate_hbm,
    taps_hbm,
    bias_hbm,
    gain_hbm,
    shift_hbm,
    residual_hbm,
    ffn_hbm,
    pick_hbm,
    logit_hbm,
    prob_hbm,
    out_hbm,
    gate_hbm,
    up_hbm,
    down_hbm,
    out_ref,
    value_ref,
    gate_ref,
    taps_ref,
    bias_ref,
    gain_ref,
    shift_ref,
    residual_ref,
    ffn_ref,
    pick_ref,
    logit_ref,
    prob_ref,
    isem,
    glued,
    hsend,
    hrecv,
    mixed,
    mrest,
    place_ref,
    meta_ref,
    normed_ref,
    proj,
    out_v,
    zsend,
    zrecv,
    mrecv,
    xsend,
    xrecv,
    asend,
    arecv,
    csend,
    cret,
    gate_v,
    up_v,
    down_v,
    hss,
    hrs,
    tss,
    trs,
    zss,
    zrs,
    mss,
    mrs,
    xss,
    xrs,
    ass,
    ars,
    css,
    crs,
):
    n_tp = lax.axis_size("tp")
    chips = lax.axis_size("sp") // PLANES
    peers = chips * n_tp
    sp = lax.axis_index("sp")
    tp = lax.axis_index("tp")
    n_sp = lax.axis_size("sp")
    z = sp // chips
    here = sp % chips
    tokens = residual_ref.shape[0]
    length, channels = value_ref.shape
    reach = taps_ref.shape[0] - 1
    lead = hsend.shape[0]
    j = here * n_tp + tp
    slots = peers * slot
    group_rows = zsend.shape[2]
    half = zsend.shape[3]

    def span(h):
        return slice(h * half, (h + 1) * half)

    def plane(d):
        if d == 1:
            return z + 1 - 2 * (z % 2)
        if d == 2:
            return z + 2 - 4 * (z // 2)
        return PLANES - 1 - z

    def mate(d):
        return (plane(d) * chips + here, tp)

    def peer(k):
        return (z * chips + k // n_tp, k % n_tp)

    def zcopy(d, h):
        return pltpu.make_async_remote_copy(
            src_ref=zsend.at[d, h], dst_ref=zrecv.at[d, h],
            send_sem=zss.at[0], recv_sem=zrs.at[d - 1, h],
            device_id=mate(d), device_id_type=MESH,
        )

    def mcopy(d):
        return pltpu.make_async_remote_copy(
            src_ref=meta_ref.at[d], dst_ref=mrecv.at[d], send_sem=mss.at[0], recv_sem=mrs.at[d - 1],
            device_id=mate(d), device_id_type=MESH,
        )

    def ccopy(d, h):
        return pltpu.make_async_remote_copy(
            src_ref=csend.at[d, h], dst_ref=cret.at[d, h],
            send_sem=css.at[0], recv_sem=crs.at[d - 1, h],
            device_id=mate(d), device_id_type=MESH,
        )

    def xcopy(d, h, o):
        rows = pl.ds(o * slot, slot)
        return pltpu.make_async_remote_copy(
            src_ref=xsend.at[d, h, rows], dst_ref=xrecv.at[d, h, rows],
            send_sem=xss.at[0], recv_sem=xrs.at[d, h],
            device_id=peer((j + o) % peers), device_id_type=MESH,
        )

    def xall(d, h):
        rows = pl.ds(slot, slots - slot)
        return pltpu.make_async_remote_copy(
            src_ref=xsend.at[d, h, rows], dst_ref=xrecv.at[d, h, rows],
            send_sem=xss.at[0], recv_sem=xrs.at[d, h],
            device_id=peer((j + 1) % peers), device_id_type=MESH,
        )

    def acopy(d, h, o):
        rows = pl.ds(o * slot, slot)
        return pltpu.make_async_remote_copy(
            src_ref=asend.at[d, h, rows], dst_ref=arecv.at[d, h, rows],
            send_sem=ass.at[0], recv_sem=ars.at[d, h],
            device_id=peer((j + peers - o) % peers), device_id_type=MESH,
        )

    def aall(d, h):
        rows = pl.ds(slot, slots - slot)
        return pltpu.make_async_remote_copy(
            src_ref=asend.at[d, h, rows], dst_ref=arecv.at[d, h, rows],
            send_sem=ass.at[0], recv_sem=ars.at[d, h],
            device_id=peer((j + peers - 1) % peers), device_id_type=MESH,
        )

    def sent(src, sem, recv_sem):
        return pltpu.make_async_remote_copy(
            src_ref=src, dst_ref=src, send_sem=sem.at[0], recv_sem=recv_sem,
            device_id=mate(1), device_id_type=MESH,
        )

    def halo():
        return pltpu.make_async_remote_copy(
            src_ref=hsend, dst_ref=hrecv, send_sem=hss.at[0], recv_sem=hrs.at[0],
            device_id=((sp + 1) % n_sp, tp), device_id_type=MESH,
        )

    wide_group = channels * n_tp // CONV_GROUPS
    block = 64

    def tcopy(o, begin, size):
        other = (tp + o) % n_tp
        rows = pl.ds(pl.multiple_of(other * tokens + begin, size), size)
        return pltpu.make_async_remote_copy(
            src_ref=mixed.at[rows], dst_ref=mrest.at[o, pl.ds(begin, size)],
            send_sem=tss.at[o - 1], recv_sem=trs.at[o - 1],
            device_id=(sp, other), device_id_type=MESH,
        )

    head_dev, tail_dev = sp == 0, sp == n_sp - 1
    barrier = pltpu.get_barrier_semaphore()
    inner = (z >= 1) & (z < PLANES - 1)
    outer = jnp.logical_not(inner)
    pl.semaphore_signal(barrier, inc=1, device_id=mate(1), device_id_type=MESH)

    @pl.when(inner)
    def _():
        pl.semaphore_signal(barrier, inc=1, device_id=mate(3), device_id_type=MESH)

    for o in range(1, peers):
        pl.semaphore_signal(
            barrier, inc=1, device_id=peer((j + o) % peers), device_id_type=MESH
        )

    @pl.when(jnp.logical_not(tail_dev))
    def _():
        pl.semaphore_signal(barrier, inc=1, device_id=(sp + 1, tp), device_id_type=MESH)

    @pl.when(jnp.logical_not(head_dev))
    def _():
        pl.semaphore_signal(barrier, inc=1, device_id=(sp - 1, tp), device_id_type=MESH)

    sources = (
        (value_hbm, value_ref), (glu_gate_hbm, gate_ref), (pick_hbm, pick_ref),
        (logit_hbm, logit_ref), (prob_hbm, prob_ref), (taps_hbm, taps_ref),
        (bias_hbm, bias_ref), (gain_hbm, gain_ref), (shift_hbm, shift_ref),
        (ffn_hbm, ffn_ref), (residual_hbm, residual_ref),
    )
    inputs = [pltpu.make_async_copy(a, b, isem.at[k]) for k, (a, b) in enumerate(sources)]
    for copy in inputs:
        copy.start()
    out_copy = pltpu.make_async_copy(out_hbm, out_v, isem.at[0])
    weights = [
        pltpu.make_async_copy(gate_hbm.at[0], gate_v, isem.at[5]),
        pltpu.make_async_copy(up_hbm.at[0], up_v, isem.at[6]),
        pltpu.make_async_copy(down_hbm.at[0], down_v, isem.at[7]),
    ]
    f32 = jnp.float32
    bf16 = jnp.bfloat16
    for copy in inputs[:2]:
        copy.wait()
    out_copy.start()
    for start in range(length - block, -1, -block):
        rows = slice(start, start + block)
        gated = value_ref[rows].astype(f32) / (1.0 + jnp.exp(-gate_ref[rows].astype(f32)))
        gated = gated.astype(bf16)
        for k in range(channels // wide_group):
            piece = gated[:, k * wide_group : (k + 1) * wide_group]
            glued[k, lead + start : lead + start + block] = piece.astype(f32)
        if start == length - block:
            hsend[...] = gated[block - lead :]
    for copy in inputs[2:5]:
        copy.wait()
    picks = pick_ref[...].astype(f32)
    logits = logit_ref[...]
    rows_of = [picks[0:1, :], picks[1:2, :], logits[0:1, :], logits[1:2, :]]
    sublane = lax.broadcasted_iota(jnp.int32, (128, tokens), 0)
    tall = jnp.zeros((128, tokens), f32)
    for k in range(2):
        tall = jnp.where(sublane == k, rows_of[k], tall)
    wide = tall.T
    cols = [wide[:, 0:1], wide[:, 1:2]]
    square = (tokens, tokens)
    earlier = lax.broadcasted_iota(jnp.int32, square, 0) < lax.broadcasted_iota(
        jnp.int32, square, 1
    )

    def group_of(pick):
        total = jnp.zeros(pick.shape, f32)
        for q in range(1, PLANES):
            total += jnp.where(pick >= (q * peers), 1.0, 0.0)
        return total

    def count(hit):
        return jnp.sum(jnp.where(hit & earlier, 1.0, 0.0), axis=0, keepdims=True)

    ranks = [count((cols[0] == r) | (cols[1] == r)) for r in rows_of[:2]]
    group_row = group_of(rows_of[0])
    spot = count(group_of(cols[0]) == group_row)
    away = group_row.astype(jnp.int32) ^ z
    at_row = away.astype(f32) * group_rows + spot
    row_id = lax.broadcasted_iota(jnp.int32, (PLANES * group_rows, tokens), 0).astype(f32)
    place_ref[...] = jnp.where(row_id == at_row, 1.0, 0.0).astype(bf16)
    gap = rows_of[2] - rows_of[3]
    shares = [prob_ref[...] / (1.0 + jnp.exp(-gap)), prob_ref[...] / (1.0 + jnp.exp(gap))]
    fields = [jnp.ones((1, tokens), f32)]
    for k in range(2):
        fields += [rows_of[k] - group_row * peers, ranks[k]]
    for share in shares:
        for _ in range(3):
            part = share.astype(bf16).astype(f32)
            fields.append(part)
            share = share - part
    field_id = lax.broadcasted_iota(jnp.int32, (16, tokens), 0)
    table = jnp.zeros((16, tokens), f32)
    for k, field in enumerate(fields):
        table = jnp.where(field_id == k, field, table)
    table = table.astype(bf16)
    meta_ref[...] = jnp.zeros(meta_ref.shape, f32)
    for d in range(PLANES):
        part = lax.dot_general(
            table,
            place_ref[d * group_rows : (d + 1) * group_rows, :],
            (((1,), (1,)), ((), ())),
            preferred_element_type=f32,
        )
        empty = (1.0 - part[0:1]) * 65536.0
        meta_ref[d, 0:1, :group_rows] = part[1:2] * slot + part[2:3] + empty
        meta_ref[d, 1:2, :group_rows] = part[3:4] * slot + part[4:5] + empty
        meta_ref[d, 2:3, :group_rows] = part[5:6] + part[6:7] + part[7:8]
        meta_ref[d, 3:4, :group_rows] = part[8:9] + part[9:10] + part[10:11]
    for copy in inputs[5:]:
        copy.wait()
    for copy in weights:
        copy.start()
    taps = taps_ref[...].astype(f32)
    def enter():
        pl.semaphore_wait(
            barrier,
            peers + jnp.where(inner, 1, 0)
            + jnp.where(head_dev, 0, 1) + jnp.where(tail_dev, 0, 1),
        )

        @pl.when(jnp.logical_not(tail_dev))
        def _():
            halo().start()

        mcopy(1).start()

        @pl.when(inner)
        def _():
            mcopy(3).start()

    spans = [(start, block) for start in range(length - block, 0, -block)]
    spans += [(block // 2, block // 2), (0, block // 2)]
    for start, size in spans:
        if start == length - block * 2:
            enter()

        if start == 0:

            @pl.when(head_dev)
            def _():
                glued[:, :lead] = jnp.zeros((channels // wide_group, lead, wide_group), f32)

            @pl.when(jnp.logical_not(head_dev))
            def _():
                halo().wait_recv()
                for k in range(channels // wide_group):
                    piece = hrecv[:, k * wide_group : (k + 1) * wide_group]
                    glued[k, :lead] = piece.astype(f32)

        for low_lane in range(0, channels, wide_group):
            part = slice(low_lane, low_lane + wide_group)
            total = jnp.zeros((size, wide_group), f32) + bias_ref[:, part]
            for offset in range(reach + 1):
                first = start + lead - reach + offset
                total += taps[offset : offset + 1, part] * glued[low_lane // wide_group, first : first + size]
            centre = jnp.mean(total, axis=-1, keepdims=True)
            total = total - centre
            variance = jnp.mean(total * total, axis=-1, keepdims=True)
            level = total * lax.rsqrt(variance + EPS)
            level = level * gain_ref[:, part] + shift_ref[:, part]
            mixed[start : start + size, part] = (level / (1.0 + jnp.exp(-level))).astype(bf16)
        if start + size == length:
            continue
        pieces = (start,) if start + size + block < length else (start, start + size)
        for piece in pieces:
            for o in range(1, n_tp):

                @pl.when((tp + o) % n_tp == piece // tokens)
                def _():
                    tcopy(o, piece % tokens, size).start()

    out_copy.wait()

    def weight_rows(which):
        return out_v[pl.ds(pl.multiple_of(which * channels, channels), channels), :]

    own = mixed[pl.ds(pl.multiple_of(tp * tokens, tokens), tokens), :]
    proj[...] = jnp.dot(own, weight_rows(tp), preferred_element_type=f32)

    for o in range(1, n_tp):
        tcopy(o, 0, tokens).wait_recv()
    for o in range(1, n_tp):
        proj[...] += jnp.dot(
            mrest[o], weight_rows((tp + n_tp - o) % n_tp), preferred_element_type=f32
        )
    for start in range(0, tokens, 16):
        rows = slice(start, start + 16)
        hidden = (residual_ref[rows].astype(f32) + proj[rows]).astype(bf16)
        full = hidden.astype(f32)
        proj[rows] = full
        scale = lax.rsqrt(jnp.mean(full * full, axis=-1, keepdims=True) + EPS)
        normed_ref[rows] = (full * scale * ffn_ref[...]).astype(bf16)

    def places(d):
        meta = meta_ref[0] if d == 0 else mrecv[d]
        row = lax.broadcasted_iota(jnp.int32, (slots, group_rows), 0).astype(jnp.float32)
        shift = (j * slot).astype(jnp.float32)
        out = []
        for k in range(2):
            at = meta[k : k + 1, :group_rows] - shift
            at = jnp.where(at < 0, at + slots, at)
            out.append(row == at)
        shares = [meta[2 + k : 3 + k, :group_rows] for k in range(2)]
        return out, shares

    def chosen(d):
        at, _ = places(d)
        return jnp.where(at[0] | at[1], 1.0, 0.0).astype(jnp.bfloat16)

    def spread(d, h, pick):
        rows = zsend[0, h] if d == 0 else zrecv[d, h]
        wide = jnp.dot(pick, rows, preferred_element_type=jnp.float32)
        wide = wide.astype(jnp.bfloat16)
        xrecv[d, h, :slot] = wide[:slot]
        xsend[d, h, slot:] = wide[slot:]
        for o in range(1, peers):
            xcopy(d, h, o).start()

    def gather(d, h):
        picked = jnp.dot(
            place_ref[d * group_rows : (d + 1) * group_rows, :],
            normed_ref[:, span(h)],
            preferred_element_type=f32,
        )
        zsend[d, h] = picked.astype(bf16)

    def dispatch(d, h):
        gather(d, h)
        if d == 1:
            zcopy(d, h).start()
        elif d == 3:

            @pl.when(inner)
            def _():
                zcopy(d, h).start()

    own_pick = chosen(0)
    for h in range(HALVES):
        gather(0, h)
        spread(0, h, own_pick)
        dispatch(3, h)
        dispatch(1, h)
    for h in range(HALVES):
        dispatch(2, h)

    def entry(d, after=(), halves=tuple(range(HALVES))):
        if halves[0] == 0:
            mcopy(d).wait_recv()
        pick = chosen(d)
        for h in halves:
            zcopy(d, h).wait_recv()
            for who in range(n_tp if after else 0):
                if h == min(who, HALVES - 1):

                    @pl.when(tp == who)
                    def _():
                        for later in after:
                            mcopy(later).start()
                            for k in range(HALVES):
                                zcopy(later, k).start()

            spread(d, h, pick)

    def expert(d):
        gate_out = None
        for h in range(HALVES):
            xall(d, h).wait_recv()
            rows = xrecv[d, h]
            gate_part = jnp.dot(rows, gate_v[span(h), :], preferred_element_type=jnp.float32)
            up_part = jnp.dot(rows, up_v[span(h), :], preferred_element_type=jnp.float32)
            gate_out = gate_part if h == 0 else gate_out + gate_part
            up_out = up_part if h == 0 else up_out + up_part
        active = (gate_out / (1.0 + jnp.exp(-gate_out)) * up_out).astype(jnp.bfloat16)
        for h in range(HALVES):
            answer = jnp.dot(active, down_v[:, span(h)], preferred_element_type=jnp.float32)
            answer = answer.astype(jnp.bfloat16)
            arecv[d, h, :slot] = answer[:slot]
            asend[d, h, slot:] = answer[slot:]

    def reply(d, halves=tuple(range(HALVES))):
        for h in halves:
            for o in range(1, peers):
                acopy(d, h, o).start()

    def settle(d, h, last=False):
        if d:
            ccopy(d, h).wait_recv()
        total = lax.dot_general(
            place_ref[d * group_rows : (d + 1) * group_rows, :],
            cret[d, h],
            (((0,), (0,)), ((), ())),
            preferred_element_type=f32,
        )
        total += proj[:, span(h)]
        if last:
            out_ref[:, span(h)] = total.astype(bf16)
        else:
            proj[:, span(h)] = total

    def combine(d, halves=tuple(range(HALVES))):
        at, shares = places(d)
        mix = jnp.where(at[0], shares[0], 0.0) + jnp.where(at[1], shares[1], 0.0)
        high = mix.astype(jnp.bfloat16)
        low = (mix - high.astype(jnp.float32)).astype(jnp.bfloat16)
        dims = (((0,), (0,)), ((), ()))
        for h in halves:
            aall(d, h).wait_recv()
            answers = arecv[d, h]
            total = lax.dot_general(high, answers, dims, preferred_element_type=jnp.float32)
            total += lax.dot_general(low, answers, dims, preferred_element_type=jnp.float32)
            if d == 0:
                cret[0, h] = total.astype(jnp.bfloat16)
            else:
                csend[d, h] = total.astype(jnp.bfloat16)
                ccopy(d, h).start()

    def drain():
        @pl.when(jnp.logical_not(tail_dev))
        def _():
            halo().wait_send()

        for o in range(1, n_tp):
            tcopy(o, 0, tokens).wait_send()
        away = pl.ds(1, PLANES - 1)
        rows = pl.ds(slot, slots - slot)
        every = pl.ds(0, HALVES)
        sent(meta_ref.at[away], mss, mrs.at[0]).wait_send()
        sent(zsend.at[away], zss, zrs.at[0, 0]).wait_send()
        sent(xsend.at[pl.ds(0, PLANES), every, rows], xss, xrs.at[0, 0]).wait_send()
        sent(asend.at[pl.ds(0, PLANES), every, rows], ass, ars.at[0, 0]).wait_send()

    head, rest = (0,), tuple(range(1, HALVES))

    @pl.when(inner)
    def _():
        entry(3, after=(2,))
        entry(1)
        for copy in weights:
            copy.wait()
        expert(0)
        expert(3)
        reply(3)
        expert(1)
        reply(1, head)
        combine(3)
        entry(2)
        reply(1, rest)
        combine(1, head)
        expert(2)
        reply(2)
        combine(1, rest)
        combine(2, head)
        reply(0)
        combine(2, rest)
        for h in range(HALVES):
            settle(3, h)
        for h in range(HALVES):
            combine(0, (h,))
            settle(0, h)
        drain()
        for h in range(HALVES):
            settle(1, h)
        for h in range(HALVES):
            settle(2, h, last=True)

    @pl.when(outer)
    def _():
        entry(1)
        for copy in weights:
            copy.wait()
        expert(0)
        entry(2, after=(3, 2))
        expert(1)
        entry(3)
        reply(1, head)
        expert(2)
        reply(2, head)
        expert(3)
        reply(3)
        combine(1, head)
        combine(2, head)
        reply(1, rest)
        reply(0, head)
        combine(3)
        reply(2, rest)
        combine(1, rest)
        reply(0, rest)
        combine(0, head)
        combine(2, rest)
        settle(0, 0)
        combine(0, rest)
        for h in rest:
            settle(0, h)
        drain()
        for h in range(HALVES):
            settle(3, h)
        settle(1, 0)
        settle(2, 0, last=True)
        for h in rest:
            settle(2, h)
            settle(1, h, last=True)

    sent(csend.at[pl.ds(1, PLANES - 1)], css, crs.at[0, 0]).wait_send()


def local(
    glu_value,
    glu_gate,
    conv_kernel,
    conv_bias,
    group_gain,
    group_shift,
    out_weight,
    residual,
    ffn_gain,
    expert_pick,
    pair_logits,
    group_prob,
    gate_weight,
    up_weight,
    down_weight,
):
    rows, width = residual.shape
    length, channels = glu_value.shape
    n_tp = lax.axis_size("tp")
    experts_all = lax.axis_size("sp") * n_tp
    cap = 4 * rows // experts_all
    peers = experts_all // PLANES
    group_rows = peers * cap // 2
    slot = max(cap, ROWS_MIN)
    slots = peers * slot
    wide_group = channels * n_tp // CONV_GROUPS
    lead = -(-(conv_kernel.shape[0] - 1) // 16) * 16
    bf16 = jnp.bfloat16
    f32 = jnp.float32
    vmem = pl.BlockSpec(memory_space=pltpu.VMEM)
    hbm = pl.BlockSpec(memory_space=pl.ANY)
    dma = pltpu.SemaphoreType.DMA
    return pl.pallas_call(
        functools.partial(layer_kernel, cap, slot),
        out_shape=pltpu.VMEM((rows, width), bf16),
        in_specs=[hbm] * 15,
        out_specs=vmem,
        scratch_shapes=[
            pltpu.VMEM(glu_value.shape, bf16),
            pltpu.VMEM(glu_gate.shape, bf16),
            pltpu.VMEM(conv_kernel.shape, bf16),
            pltpu.VMEM((1, channels), f32),
            pltpu.VMEM((1, channels), f32),
            pltpu.VMEM((1, channels), f32),
            pltpu.VMEM((rows, width), bf16),
            pltpu.VMEM((1, width), f32),
            pltpu.VMEM((2, rows), jnp.int32),
            pltpu.VMEM((2, rows), f32),
            pltpu.VMEM((1, rows), f32),
            dma((11,)),
            pltpu.VMEM((channels // wide_group, lead + length, wide_group), f32),
            pltpu.VMEM((lead, channels), bf16),
            pltpu.VMEM((lead, channels), bf16),
            pltpu.VMEM((length, channels), bf16),
            pltpu.VMEM((n_tp, rows, channels), bf16),
            pltpu.VMEM((PLANES * group_rows, rows), bf16),
            pltpu.VMEM((PLANES, 8, 128), f32),
            pltpu.VMEM((rows, width), bf16),
            pltpu.VMEM((rows, width), f32),
            pltpu.VMEM(out_weight.shape, bf16),
            pltpu.VMEM((PLANES, HALVES, group_rows, width // HALVES), bf16),
            pltpu.VMEM((PLANES, HALVES, group_rows, width // HALVES), bf16),
            pltpu.VMEM((PLANES, 8, 128), f32),
            pltpu.VMEM((PLANES, HALVES, slots, width // HALVES), bf16),
            pltpu.VMEM((PLANES, HALVES, slots, width // HALVES), bf16),
            pltpu.VMEM((PLANES, HALVES, slots, width // HALVES), bf16),
            pltpu.VMEM((PLANES, HALVES, slots, width // HALVES), bf16),
            pltpu.VMEM((PLANES, HALVES, group_rows, width // HALVES), bf16),
            pltpu.VMEM((PLANES, HALVES, group_rows, width // HALVES), bf16),
            pltpu.VMEM(gate_weight.shape[1:], bf16),
            pltpu.VMEM(up_weight.shape[1:], bf16),
            pltpu.VMEM(down_weight.shape[1:], bf16),
            dma((1,)),
            dma((1,)),
            dma((n_tp - 1,)),
            dma((n_tp - 1,)),
            dma((1,)),
            dma((PLANES - 1, HALVES)),
            dma((1,)),
            dma((PLANES - 1,)),
            dma((1,)),
            dma((PLANES, HALVES)),
            dma((1,)),
            dma((PLANES, HALVES)),
            dma((1,)),
            dma((PLANES - 1, HALVES)),
        ],
        compiler_params=pltpu.CompilerParams(
            collective_id=0, has_side_effects=True, vmem_limit_bytes=62 * 1024 * 1024
        ),
    )(
        glu_value,
        glu_gate,
        conv_kernel,
        conv_bias[None, :],
        group_gain[None, :],
        group_shift[None, :],
        residual,
        ffn_gain[None, :],
        expert_pick.T,
        pair_logits.T,
        group_prob[None, :],
        out_weight,
        gate_weight,
        up_weight,
        down_weight,
    )


def solution(mesh):
    in_specs = (
        P("sp", "tp"),
        P("sp", "tp"),
        P(None, "tp"),
        P("tp"),
        P("tp"),
        P("tp"),
        P(),
        P(("sp", "tp"), None),
        P(),
        P(("sp", "tp"), None),
        P(("sp", "tp"), None),
        P(("sp", "tp")),
        P(("sp", "tp"), None, None),
        P(("sp", "tp"), None, None),
        P(("sp", "tp"), None, None),
    )
    out_specs = P(("sp", "tp"), None)
    return jax.shard_map(local, mesh=mesh, in_specs=in_specs, out_specs=out_specs, check_vma=False)
```
